32 devices in a mesh: rep: 8 (over z, y), fs: 2 (over x), tp: 2 (over core).
Axes of the slice: x: 2, y: 2, z: 4, core: 2. Of those that a mesh axis runs over, the one named last changes fastest.
Arguments:
- inputs: bfloat16 [4096, 2048], P(('rep', 'tp'), 'fs'), may hold values from -6 to 6
- pre_act: bfloat16 [4096, 4096], P(('rep', 'fs'), 'tp'), may hold values from -6 to 6
- cotangent: bfloat16 [4096, 2048], P(('rep', 'tp'), 'fs'), may hold values from -6 to 6
- up_weight: bfloat16 [2048, 4096], P('fs', 'tp'), may hold values from -0.125 to 0.125
- down_weight: bfloat16 [4096, 2048], P('tp', 'fs'), may hold values from -0.09375 to 0.09375
Outputs:
- grad_inputs: bfloat16 [4096, 2048], P(('rep', 'tp'), 'fs')
- grad_up: float32 [2048, 4096], P('fs', 'tp')
- grad_down: float32 [4096, 2048], P('tp', 'fs')
The draws below stay inside these ranges and needn't reach their ends.
All inputs are finite; a program needn't handle non-finite values.
Results may differ from the reference program's by a relative error of at most 0.015.
Values may be sent and summed in bfloat16 or wider, within the bound.
A program may use at most 128 MiB of HBM per device.

```python
import jax
import jax.numpy as jnp
from jax import lax

D = 2048
FF = 4096
TOKENS = 4096
N_TP = 2


def raised(array, rng, source, target, parts, factor):
    owner, partner = [(jnp.arange(array.shape[position]) // (array.shape[position] // parts)).reshape([-1 if axis == position else 1 for axis in range(array.ndim)]) for position in (source, target)]
    chosen = jax.random.permutation(rng, parts)[partner]
    strong = (owner == chosen) | (owner == (partner + parts // 2) % parts)
    return jnp.where(strong, factor * array, array)


def block_levels(stream_key, shape, shards, low, top_value):
    def one(dim, blocks):
        heights = jax.random.uniform(jax.random.fold_in(jax.random.fold_in(stream_key, 6), dim), (blocks,), jnp.float32, low / len(shards), top_value / len(shards))
        return jnp.repeat(jnp.exp(heights), shape[dim] // blocks).reshape((-1,) + (1,) * (len(shape) - dim - 1))

    level = one(*shards[0])
    for cut in shards[1:]:
        level = level * one(*cut)
    return level


def bell_draw(key, dims, scale, reach, pieces=(), held_as=jnp.bfloat16):
    values = jax.random.normal(key, dims, jnp.float32) * scale
    if len(pieces) > 0:
        values = block_levels(key, dims, pieces, -0.22, 0.18) * values
    return jnp.clip(values, min=-reach, max=reach).astype(held_as)


def bell_draw_with(rng, shape, spread, limit, split, heavy, dtype=jnp.bfloat16):
    entries = spread * jax.random.normal(rng, shape, jnp.float32)
    if split:
        entries = entries * block_levels(rng, shape, split, -0.22, 0.18)
    return jnp.clip(raised(entries, jax.random.fold_in(rng, 3), *heavy), -limit, limit).astype(dtype)


def setup_inputs(seed: int = 0) -> dict:
    splits = jax.random.split(jax.random.key(seed), 6)
    return {
        "inputs": bell_draw(splits[0], (TOKENS, D), 1.0, 6.0, ((0, 16), (1, 2))),
        "pre_act": bell_draw(splits[1], (TOKENS, FF), 1.0, 6.0, ((0, 16), (1, 2))),
        "cotangent": bell_draw_with(splits[2], (TOKENS, D), 1.0, 6.0, ((0, 16), (1, 2)), (0, 1, 16, 2.0)),
        "up_weight": bell_draw(splits[3], (D, FF), D ** -0.5, 0.125, ((0, 2), (1, 2))),
        "down_weight": bell_draw(splits[4], (FF, D), FF ** -0.5, 0.09375, ((0, 2), (1, 2))),
    }


def reference(inputs, pre_act, cotangent, up_weight, down_weight):
    positive = jnp.maximum(pre_act.astype(jnp.float32), 0.0)
    square = (positive * positive).astype(jnp.bfloat16)
    grad_act = jnp.dot(cotangent, down_weight.T, preferred_element_type=jnp.float32)
    grad_pre = (2.0 * positive * grad_act).astype(jnp.bfloat16)
    factor = TOKENS ** -0.5
    grad_down = jnp.dot(square.T, cotangent, preferred_element_type=jnp.float32) * factor
    grad_up = jnp.dot(inputs.T, grad_pre, preferred_element_type=jnp.float32) * factor
    width = FF // N_TP
    total = jnp.zeros(inputs.shape, jnp.float32)
    for block in range(N_TP):
        partial_sum = jnp.dot(grad_pre[:, block * width:(block + 1) * width],
                              up_weight[:, block * width:(block + 1) * width].T,
                              preferred_element_type=jnp.float32).astype(jnp.bfloat16)
        partial_sum = lax.optimization_barrier(partial_sum)
        total = total + partial_sum.astype(jnp.float32)
    grad_inputs = total.astype(jnp.bfloat16)
    return grad_inputs, grad_up, grad_down
```

```python
import functools

import jax
import jax.numpy as jnp
from jax import lax
from jax.experimental import pallas as pl
from jax.experimental.pallas import tpu as pltpu
from jax.sharding import PartitionSpec as P

MESH = pl.DeviceIdType.MESH
LANES = 128
F32, BF16 = jnp.float32, jnp.bfloat16

ACT, GRAD, HOP, CROSS, SPREAD, TAKE = 4, 2, 1, 1, 3, 8


def rows_dot(left, right):
    return lax.dot_general(left, right, (((0,), (0,)), ((), ())), preferred_element_type=F32)


def cols_dot(left, right):
    return lax.dot_general(left, right, (((1,), (1,)), ((), ())), preferred_element_type=F32)


def kernel(
    n_rep, x_hbm, pre_hbm, cot_hbm, wu_hbm, wd_hbm,
    gi_ref, up_ref, res,
    pre_ref, wu, wd, tok, hid, pa_own, pa_out, pa_in, gi_out, gi_in, part, out, inc,
    w_sem, tp_s, tp_r, yt_s, yt_r, ya_s, ya_r, ox_s, ox_r, fx_s, fx_r, gx_s, gx_r,
    pa_s, pa_r, gi_s, gi_r, rs_s, rs_r, fc_s, fo_s, fz_r, fy_s, fy_r,
):
    half, hidden = pre_ref.shape
    width = wd.shape[1]
    panels = hidden // LANES
    sub = LANES // 2
    rep, fs, tp = lax.axis_index("rep"), lax.axis_index("fs"), lax.axis_index("tp")
    rows_n = n_rep // 2
    mid = rows_n // 2
    row, col = rep // 2, rep % 2
    side = jnp.where(row >= mid, 1, 0)
    depth = jnp.where(row >= mid, row - mid, mid - 1 - row)
    has_outer = depth < mid - 1
    middle = depth == 0
    step = 2 * side - 1

    def rep_at(r):
        return 2 * lax.rem(r + rows_n, rows_n) + col

    outer, inner = {"rep": rep_at(row + step)}, {"rep": rep_at(row - step)}
    other_y = {"rep": 2 * row + 1 - col}
    other_fs, other_tp = {"fs": 1 - fs}, {"tp": 1 - tp}

    def block(c, b):
        return pl.ds(pl.multiple_of((2 * c + b) * half, half), half)

    own_f, own_hf = block(col, fs), block(col, 1 - fs)
    far_f, far_hf = block(1 - col, fs), block(1 - col, 1 - fs)
    own_t, own_ht = block(col, tp), block(col, 1 - tp)
    far_t, far_ht = block(1 - col, tp), block(1 - col, 1 - tp)

    def remote(src, dst, s, r, dev):
        return pltpu.make_async_remote_copy(
            src_ref=src, dst_ref=dst, send_sem=s, recv_sem=r, device_id=dev,
            device_id_type=MESH)

    barrier = pltpu.get_barrier_semaphore()
    for dev in (outer, inner, other_y, other_fs, other_tp):
        pl.semaphore_signal(barrier, inc=1, device_id=dev, device_id_type=MESH)
    held = ((cot_hbm, tok.at[1, own_t]), (x_hbm, tok.at[0, own_t]), (pre_hbm, pre_ref),
            (wd_hbm, wd), (wu_hbm, wu))
    loads = [pltpu.make_async_copy(src, dst, w_sem.at[i]) for i, (src, dst) in enumerate(held)]
    load_cot, load_x, load_pre, load_wd, load_wu = loads
    for load in loads:
        load.start()
    load_cot.wait()
    load_x.wait()
    pl.semaphore_wait(barrier, 5)

    def lanes(k):
        return pl.ds(pl.multiple_of(k * LANES, LANES), LANES)

    def rows(k, s):
        return pl.ds(pl.multiple_of(k * LANES + s * sub, sub), sub)

    def moved(ref, at, s, r, dev):
        return remote(ref.at[at], ref.at[at], s, r, dev)

    y_move = moved(tok, (1 - col, own_t), yt_s, yt_r, other_y)
    y_move.start()
    cot_move = moved(tok, (1, own_t), tp_s.at[0], tp_r.at[0], other_tp)
    cot_move.start()
    x_move = moved(tok, (0, own_t), tp_s.at[1], tp_r.at[1], other_tp)
    far_move = moved(tok, (col, far_t), tp_s.at[2], tp_r.at[2], other_tp)

    @pl.when(col == 0)
    def _():
        x_move.start()

    def ya_copy(k):
        return moved(hid, (1 - col, own_f, lanes(k)), ya_s.at[k], ya_r.at[k], other_y)

    def ox_copy(k):
        return moved(hid, (col, own_f, lanes(k)), ox_s.at[k], ox_r.at[k], other_fs)

    def fx_copy(k):
        return moved(hid, (col, far_f, lanes(k)), fx_s.at[k], fx_r.at[k], other_fs)

    def gx_copy(k):
        return moved(hid, (0, own_f, lanes(k)), gx_s.at[k], gx_r.at[k], other_fs)

    def pa_copy(k):
        return remote(pa_out.at[:, lanes(k)], pa_in.at[:, lanes(k)], pa_s.at[k], pa_r.at[k],
                      other_fs)

    load_pre.wait()

    def own_square(k, _):
        positive = jnp.maximum(pre_ref[:, lanes(k)].astype(F32), 0.0)
        hid[1, own_f, lanes(k)] = (positive * positive).astype(BF16)

        @pl.when(col == 0)
        def _():
            ya_copy(k).start()
        return 0
    lax.fori_loop(0, panels, own_square, 0)
    load_wd.wait()
    cot_move.wait_recv()

    def act(k):
        pa_out[:, lanes(k)] = cols_dot(tok[1, own_hf, :], wd[lanes(k), :]).astype(BF16)
        pa_copy(k).start()

        @pl.when(col == 1)
        def _():
            ox_copy(k).start()
        pa_own[:, lanes(k)] = cols_dot(tok[1, own_f, :], wd[lanes(k), :])

    def grad(k):
        pa_copy(k).wait_recv()
        positive = jnp.maximum(pre_ref[:, lanes(k)].astype(F32), 0.0)
        total = pa_own[:, lanes(k)] + pa_in[:, lanes(k)].astype(F32)
        hid[0, own_f, lanes(k)] = (2.0 * positive * total).astype(BF16)

        @pl.when(col == 0)
        def _():
            ox_copy(k).start()

        @pl.when(col == 1)
        def _():
            ya_copy(k).start()

    def hop(k):
        remote(hid.at[1 - col, own_f, lanes(k)], hid.at[col, far_f, lanes(k)], ya_s.at[k],
               ya_r.at[k], other_y).wait_recv()
        fx_copy(k).start()

    def rs_copy(k, s):
        slot = jnp.where(middle, 1, 0)
        return remote(out.at[rows(k, s)], inc.at[slot, rows(k, s)], rs_s.at[k, s],
                      rs_r.at[slot, k, s], inner)

    def rs_wait(slot, k, s):
        remote(out.at[rows(k, s)], inc.at[slot, rows(k, s)], rs_s.at[k, s],
               rs_r.at[slot, k, s], inner).wait_recv()

    def final(k, s, sem, dev):
        return moved(res, (col, rows(k, s)), sem, fz_r.at[k, s], dev)

    def final_y(k, s):
        return moved(res, (col, rows(k, s)), fy_s.at[k, s], fy_r.at[k, s], other_y)

    def reduce(k):
        ox_copy(k).wait_recv()
        fx_copy(k).wait_recv()
        part[...] = rows_dot(hid[col, :, lanes(k)], tok[col])
        for s in (1 - side, side):
            mine = part[pl.ds(pl.multiple_of(s * sub, sub), sub), :]

            @pl.when(has_outer)
            def _():
                rs_wait(0, k, s)
                out[rows(k, s), :] = (mine + inc[0, rows(k, s), :].astype(F32)).astype(BF16)

            @pl.when(jnp.logical_not(has_outer))
            def _():
                out[rows(k, s), :] = mine.astype(BF16)

            if s is side:
                @pl.when(jnp.logical_not(middle))
                def _():
                    rs_copy(k, s).start()
            else:
                rs_copy(k, s).start()

    def spread(k, s):
        @pl.when(has_outer)
        def _():
            final(k, s, fo_s.at[k, s], outer).start()
        final_y(k, s).start()

    def cross(k):
        @pl.when(middle)
        def _():
            at = rows(k, side)
            rs_wait(1, k, side)
            res[col, at, :] = (out[at, :].astype(F32) + inc[1, at, :].astype(F32)).astype(BF16)
            final(k, side, fc_s.at[k], inner).start()
            spread(k, side)

    def forward(k):
        final(k, 1 - side, fc_s.at[k], inner).wait_recv()
        spread(k, 1 - side)

        @pl.when(jnp.logical_not(middle))
        def _():
            final(k, side, fc_s.at[k], inner).wait_recv()
            spread(k, side)

    def take(k):
        for s in range(2):
            moved(res, (1 - col, rows(k, s)), fy_s.at[k, s], fy_r.at[k, s], other_y).wait_recv()
        up_ref[:, lanes(k)] = res[0, lanes(k), :].T

    def early(k, _):
        act(k)
        return 0
    lax.fori_loop(0, ACT, early, 0)

    def early_grad(k, _):
        grad(k)
        return 0
    lax.fori_loop(0, GRAD, early_grad, 0)
    remote(tok.at[1 - col, own_t], tok.at[col, far_t], yt_s, yt_r, other_y).wait_recv()
    far_move.start()

    @pl.when(col == 0)
    def _():
        x_move.wait_recv()

    def early_hop(k, _):
        hop(k)
        return 0
    lax.fori_loop(0, HOP, early_hop, 0)
    far_move.wait_recv()

    def main(i, _):
        @pl.when(i + ACT < panels)
        def _():
            act(i + ACT)

        @pl.when(i + GRAD < panels)
        def _():
            grad(i + GRAD)

        @pl.when(i + HOP < panels)
        def _():
            hop(i + HOP)
        reduce(i)

        @pl.when(i >= CROSS)
        def _():
            cross(i - CROSS)

        @pl.when(i >= SPREAD)
        def _():
            forward(i - SPREAD)

        @pl.when((col == 1) & (i >= panels // 2))
        def _():
            for n in range(2):
                gx_copy(2 * (i - panels // 2) + n).start()

        @pl.when(i >= TAKE)
        def _():
            take(i - TAKE)
        return 0
    lax.fori_loop(0, panels, main, 0)
    load_wu.wait()
    cross(panels - 1)
    forward(panels - 3)

    @pl.when(col == 1)
    def _():
        def gx_wait(k, _):
            gx_copy(k).wait_recv()
            return 0
        lax.fori_loop(0, panels, gx_wait, 0)

    wide = min(2 * LANES, width)

    def input_out(n, _):
        at = pl.ds(pl.multiple_of(n * wide, wide), wide)
        gi_out[:, at] = cols_dot(hid[0, own_ht, :], wu[at, :]).astype(BF16)
        return 0
    lax.fori_loop(0, width // wide, input_out, 0)
    gi_move = remote(gi_out, gi_in, gi_s, gi_r, other_tp)
    gi_move.start()
    forward(panels - 2)

    def late(k, _):
        take(k)
        return 0
    lax.fori_loop(panels - TAKE, panels - 5, late, 0)
    forward(panels - 1)

    def input_own(n, _):
        at = pl.ds(pl.multiple_of(n * wide, wide), wide)
        mine = cols_dot(hid[0, own_t, :], wu[at, :]).astype(BF16).astype(F32)
        gi_ref[:, at] = mine.astype(BF16)
        return 0
    lax.fori_loop(0, width // wide, input_own, 0)
    gi_move.wait_recv()
    gi_ref[...] = (gi_ref[...].astype(F32) + gi_in[...].astype(F32)).astype(BF16)
    lax.fori_loop(panels - 5, panels, late, 0)

    for move in (y_move, cot_move, far_move, gi_move):
        move.wait_send()

    @pl.when(col == 0)
    def _():
        x_move.wait_send()

    def sent(k, _):
        for copy in (pa_copy, ya_copy, ox_copy, fx_copy):
            copy(k).wait_send()

        @pl.when(col == 1)
        def _():
            gx_copy(k).wait_send()

        rs_copy(k, 1 - side).wait_send()

        @pl.when(middle)
        def _():
            final(k, side, fc_s.at[k], inner).wait_send()

        @pl.when(jnp.logical_not(middle))
        def _():
            rs_copy(k, side).wait_send()
        for s in range(2):
            final_y(k, s).wait_send()

            @pl.when(has_outer)
            def _():
                final(k, s, fo_s.at[k, s], outer).wait_send()
        return 0
    lax.fori_loop(0, panels, sent, 0)


def scale_kernel(factor, pieces, gi, up, res, gi_out, up_out, down_out, up_wide, down_wide,
                 sems, gi_sem):
    copies = [pltpu.make_async_copy(gi, gi_out, gi_sem)]
    copies[0].start()
    for i in range(pieces):
        for n, (src, wide, dst) in enumerate(
                ((up, up_wide, up_out), (res.at[1], down_wide, down_out))):
            rows = pl.ds(i * (src.shape[0] // pieces), src.shape[0] // pieces)
            wide[rows, :] = src[rows, :].astype(F32) * factor
            copy = pltpu.make_async_copy(wide.at[rows, :], dst.at[rows, :], sems.at[n, i])
            copy.start()
            copies.append(copy)
    for copy in copies:
        copy.wait()


def per_device(n_rep, inputs, pre_act, cotangent, up_weight, down_weight):
    half, width = inputs.shape
    hidden = pre_act.shape[1]
    panels = hidden // LANES
    dma = pltpu.SemaphoreType.DMA
    vmem = pl.BlockSpec(memory_space=pltpu.VMEM)
    anywhere = pl.BlockSpec(memory_space=pl.ANY)
    one, two = dma((panels,)), dma((panels, 2))
    grad_inputs, grad_up, result = pl.pallas_call(
        functools.partial(kernel, n_rep),
        name="ffn_backward",
        out_shape=(
            pltpu.VMEM((half, width), BF16),
            pltpu.VMEM((width, hidden), BF16),
            pltpu.VMEM((2, hidden, width), BF16),
        ),
        in_specs=[anywhere] * 5,
        out_specs=(vmem, vmem, vmem),
        scratch_shapes=[
            pltpu.VMEM((half, hidden), BF16),
            pltpu.VMEM((width, hidden), BF16),
            pltpu.VMEM((hidden, width), BF16),
            pltpu.VMEM((2, 4 * half, width), BF16),
            pltpu.VMEM((2, 4 * half, hidden), BF16),
            pltpu.VMEM((half, hidden), F32),
            pltpu.VMEM((half, hidden), BF16),
            pltpu.VMEM((half, hidden), BF16),
            pltpu.VMEM((half, width), BF16),
            pltpu.VMEM((half, width), BF16),
            pltpu.VMEM((LANES, width), F32),
            pltpu.VMEM((hidden, width), BF16),
            pltpu.VMEM((2, hidden, width), BF16),
            dma((5,)), dma((3,)), dma((3,)), dma, dma,
            one, one, one, one, one, one, one, one,
            one, one, dma, dma,
            two, dma((2, panels, 2)), one, two, two, two, two,
        ],
        compiler_params=pltpu.CompilerParams(
            collective_id=0, has_side_effects=True, vmem_limit_bytes=48 * 2**20
        ),
    )(inputs, pre_act, cotangent, up_weight, down_weight)
    factor = (half * n_rep * lax.axis_size("tp")) ** (-0.5)
    pieces = 8
    return pl.pallas_call(
        functools.partial(scale_kernel, factor, pieces),
        name="scale_outputs",
        out_shape=(
            jax.ShapeDtypeStruct((half, width), BF16),
            jax.ShapeDtypeStruct((width, hidden), F32),
            jax.ShapeDtypeStruct((hidden, width), F32),
        ),
        in_specs=[vmem] * 3,
        out_specs=[anywhere] * 3,
        scratch_shapes=[
            pltpu.VMEM((width, hidden), F32),
            pltpu.VMEM((hidden, width), F32),
            dma((2, pieces)),
            dma,
        ],
        compiler_params=pltpu.CompilerParams(vmem_limit_bytes=40 * 2**20),
    )(*[pltpu.with_memory_space_constraint(g, pltpu.VMEM)
        for g in (grad_inputs, grad_up, result)])


def solution(mesh):
    assert mesh.shape["fs"] == 2 and mesh.shape["tp"] == 2 and mesh.shape["rep"] % 4 == 0
    placed = (
        P(("rep", "tp"), "fs"),
        P(("rep", "fs"), "tp"),
        P(("rep", "tp"), "fs"),
        P("fs", "tp"),
        P("tp", "fs"),
    )
    return jax.shard_map(
        functools.partial(per_device, mesh.shape["rep"]),
        mesh=mesh,
        in_specs=placed,
        out_specs=(P(("rep", "tp"), "fs"), P("fs", "tp"), P("tp", "fs")),
        check_vma=False,
    )
```

```python
import functools

import jax
import jax.numpy as jnp
from jax import lax
from jax.experimental import pallas as pl
from jax.experimental.pallas import tpu as pltpu
from jax.sharding import PartitionSpec as P

MESH = pl.DeviceIdType.MESH
LANES = 128
F32, BF16 = jnp.float32, jnp.bfloat16

FIRST, START, MORE, HOP, PACE = 4, 2, 5, 2, 3
CROSS, SPREAD, APART, TAKE = 2, 4, 4, 6


def rows_dot(left, right):
    return lax.dot_general(left, right, (((0,), (0,)), ((), ())), preferred_element_type=F32)


def cols_dot(left, right):
    return lax.dot_general(left, right, (((1,), (1,)), ((), ())), preferred_element_type=F32)


def kernel(
    n_rep, x_hbm, pre_hbm, cot_hbm, wu_hbm, wd_hbm,
    gi_ref, up_ref, res,
    pre_ref, wu, wd, tok, hid, pa_own, pa_out, pa_in, gi_out, gi_in, part, out, inc,
    w_sem, tp_s, tp_r, yt_s, yt_r, ya_s, ya_r, ox_s, fx_s, act_r, gx_s, gx_r,
    pa_s, pa_r, gi_s, gi_r, rs_s, rs_r, fc_s, fo_s, fz_r, fy_s, fy_r,
):
    half, hidden = pre_ref.shape
    width = wd.shape[1]
    panels = hidden // LANES
    sub, wide = LANES // 2, width // 2
    chunks = 2 * panels
    rep, fs, tp = lax.axis_index("rep"), lax.axis_index("fs"), lax.axis_index("tp")
    rows_n = n_rep // 2
    mid = rows_n // 2
    row, col = rep // 2, rep % 2
    side = jnp.where(row >= mid, 1, 0)
    depth = jnp.where(row >= mid, row - mid, mid - 1 - row)
    has_outer = depth < mid - 1
    middle = depth == 0
    step = 2 * side - 1

    def rep_at(r):
        return 2 * lax.rem(r + rows_n, rows_n) + col

    outer, inner = {"rep": rep_at(row + step)}, {"rep": rep_at(row - step)}
    other_y = {"rep": 2 * row + 1 - col}
    other_fs, other_tp = {"fs": 1 - fs}, {"tp": 1 - tp}

    def block(c, b):
        return pl.ds(pl.multiple_of((2 * c + b) * half, half), half)

    own_f, own_hf = block(col, fs), block(col, 1 - fs)
    far_f, far_hf = block(1 - col, fs), block(1 - col, 1 - fs)
    own_t, own_ht = block(col, tp), block(col, 1 - tp)
    far_t, far_ht = block(1 - col, tp), block(1 - col, 1 - tp)

    def remote(src, dst, s, r, dev):
        return pltpu.make_async_remote_copy(
            src_ref=src, dst_ref=dst, send_sem=s, recv_sem=r, device_id=dev,
            device_id_type=MESH)

    barrier = pltpu.get_barrier_semaphore()
    for dev in (outer, inner, other_y, other_fs, other_tp):
        pl.semaphore_signal(barrier, inc=1, device_id=dev, device_id_type=MESH)
    held = ((cot_hbm, tok.at[1, own_t]), (x_hbm, tok.at[0, own_t]), (pre_hbm, pre_ref),
            (wd_hbm, wd), (wu_hbm, wu))
    loads = [pltpu.make_async_copy(src, dst, w_sem.at[i]) for i, (src, dst) in enumerate(held)]
    load_cot, load_x, load_pre, load_wd, load_wu = loads
    for load in loads:
        load.start()
    load_cot.wait()
    load_x.wait()
    pl.semaphore_wait(barrier, 5)

    def lanes(k):
        return pl.ds(pl.multiple_of(k * LANES, LANES), LANES)

    def where_is(k):
        early = k < 4
        return jnp.where(early, k % 2, k // 2), jnp.where(early, k // 2, k % 2)

    def cols(w):
        return pl.ds(pl.multiple_of(w * wide, wide), wide)

    def piece(k, s):
        p, w = where_is(k)
        return pl.ds(pl.multiple_of(p * LANES + s * sub, sub), sub), cols(w)

    def moved(ref, at, s, r, dev):
        return remote(ref.at[at], ref.at[at], s, r, dev)

    def y_move(w):
        return moved(tok, (1 - col, own_t, cols(w)), yt_s.at[w], yt_r.at[w], other_y)

    def far_move(w):
        return moved(tok, (col, far_t, cols(w)), tp_s.at[2 + w], tp_r.at[2 + w], other_tp)

    y_move(0).start()
    cot_move = moved(tok, (1, own_t), tp_s.at[0], tp_r.at[0], other_tp)
    cot_move.start()
    x_move = moved(tok, (0, own_t), tp_s.at[1], tp_r.at[1], other_tp)

    @pl.when(col == 0)
    def _():
        x_move.start()

    def ya_copy(k):
        return moved(hid, (1 - col, own_f, lanes(k)), ya_s, ya_r.at[k], other_y)

    def ox_copy(k):
        return moved(hid, (col, own_f, lanes(k)), ox_s, act_r.at[k], other_fs)

    def fx_copy(k):
        return moved(hid, (col, far_f, lanes(k)), fx_s, act_r.at[k], other_fs)

    def gx_copy(k):
        return moved(hid, (0, own_f, lanes(k)), gx_s, gx_r, other_fs)

    def pa_copy(k):
        return remote(pa_out.at[:, lanes(k)], pa_in.at[:, lanes(k)], pa_s, pa_r.at[k],
                      other_fs)

    load_pre.wait()

    def each(lo, hi, body):
        def once(k, _):
            body(k)
            return 0
        lax.fori_loop(lo, hi, once, 0)

    def own_square(k):
        positive = jnp.maximum(pre_ref[:, lanes(k)].astype(F32), 0.0)
        hid[1, own_f, lanes(k)] = (positive * positive).astype(BF16)

        @pl.when(col == 0)
        def _():
            ya_copy(k).start()

    each(0, 2, own_square)

    @pl.when(col == 0)
    def _():
        y_move(1).start()
    each(2, panels, own_square)
    load_wd.wait()
    cot_move.wait_recv()

    def act(k):
        pa_out[:, lanes(k)] = cols_dot(tok[1, own_hf, :], wd[lanes(k), :]).astype(BF16)
        pa_copy(k).start()
        pa_own[:, lanes(k)] = cols_dot(tok[1, own_f, :], wd[lanes(k), :])

    def pair(k):
        ox_copy(k).start()

    def grad(k):
        pa_copy(k).wait_recv()
        positive = jnp.maximum(pre_ref[:, lanes(k)].astype(F32), 0.0)
        total = pa_own[:, lanes(k)] + pa_in[:, lanes(k)].astype(F32)
        hid[0, own_f, lanes(k)] = (2.0 * positive * total).astype(BF16)

        @pl.when(col == 1)
        def _():
            ya_copy(k).start()

    def hop(k):
        remote(hid.at[1 - col, own_f, lanes(k)], hid.at[col, far_f, lanes(k)], ya_s,
               ya_r.at[k], other_y).wait_recv()
        fx_copy(k).start()

    def rs_copy(k, s):
        slot = jnp.where(middle, 1, 0)
        return remote(out.at[piece(k, s)], inc.at[(slot, *piece(k, s))], rs_s,
                      rs_r.at[jnp.where(middle, 2, s), k], inner)

    def rs_wait(slot, k, s):
        remote(out.at[piece(k, s)], inc.at[(slot, *piece(k, s))], rs_s,
               rs_r.at[2 if slot else s, k], inner).wait_recv()

    def final(k, s, sem, dev):
        return moved(res, (col, *piece(k, s)), sem, fz_r.at[k, s], dev)

    def final_y(k, s):
        return moved(res, (col, *piece(k, s)), fy_s, fy_r.at[k], other_y)

    def arrive(k):
        moved(hid, (col, pl.ds(0, 2 * half), lanes(k)), ox_s, act_r.at[k], other_fs).wait_recv()

    def reduce(k):
        p, w = where_is(k)
        part[...] = rows_dot(hid[col, :, lanes(p)], tok[col, :, cols(w)])
        for s in (1 - side, side):
            at = piece(k, s)
            mine = part[pl.ds(pl.multiple_of(s * sub, sub), sub), :]

            @pl.when(has_outer)
            def _():
                rs_wait(0, k, s)
                out[at] = (mine + inc[(0, *at)].astype(F32)).astype(BF16)

            @pl.when(jnp.logical_not(has_outer))
            def _():
                out[at] = mine.astype(BF16)

            if s is side:
                @pl.when(jnp.logical_not(middle))
                def _():
                    rs_copy(k, s).start()
            else:
                rs_copy(k, s).start()

    def spread(k, s):
        @pl.when(has_outer)
        def _():
            final(k, s, fo_s, outer).start()
        final_y(k, s).start()

    def cross(k):
        @pl.when(middle)
        def _():
            at = piece(k, side)
            rs_wait(1, k, side)
            res[(col, *at)] = (out[at].astype(F32) + inc[(1, *at)].astype(F32)).astype(BF16)
            final(k, side, fc_s, inner).start()
            spread(k, side)

    def forward(k):
        final(k, 1 - side, fc_s, inner).wait_recv()
        spread(k, 1 - side)

        @pl.when(jnp.logical_not(middle))
        def _():
            final(k, side, fc_s, inner).wait_recv()
            spread(k, side)

    def take(k):
        p, w = where_is(k)
        at = (lanes(p), cols(w))
        moved(res, (1 - col, *at), fy_s, fy_r.at[k], other_y).wait_recv()
        up_ref[cols(w), lanes(p)] = res[(0, *at)].T

    def when_in(i, end, body):
        @pl.when((i >= 0) & (i < end))
        def _():
            body(i)

    each(0, FIRST, act)

    def ready(k):
        grad(k)
        pair(k)
    each(0, START, ready)

    @pl.when(col == 1)
    def _():
        y_move(1).start()
    act(FIRST)
    more = FIRST + 1 + MORE

    def far_arrived(w):
        remote(tok.at[1 - col, own_t, cols(w)], tok.at[col, far_t, cols(w)], yt_s.at[w],
               yt_r.at[w], other_y).wait_recv()
        far_move(w).start()

    far_arrived(0)

    @pl.when(col == 0)
    def _():
        x_move.wait_recv()

    each(0, HOP, hop)
    far_move(0).wait_recv()
    each(FIRST + 1, more, act)
    each(START, START + PACE, grad)

    furthest = SPREAD + APART * (mid - 1)
    take_lag = furthest + TAKE

    def spreading(k):
        when_in(k - CROSS, chunks, cross)
        when_in(k - SPREAD - APART * depth, chunks, forward)
        when_in(k - take_lag, chunks, take)

    def main(i):
        @pl.when(i == 1)
        def _():
            far_arrived(1)
            far_move(1).wait_recv()
        for n in range(2):
            @pl.when(i == 0)
            def _():
                arrive(n)
            if n == 0:
                @pl.when(i > 1)
                def _():
                    arrive(i)
            reduce(2 * i + n)

            if n == 0:
                for step in range(PACE):
                    when_in(more + PACE * i + step, panels, act)
                    when_in(START + PACE + PACE * i + step, panels, grad)
                when_in(i + HOP, panels, pair)
                when_in(i + HOP, panels, hop)
            spreading(2 * i + n)

        @pl.when((col == 1) & (i >= panels // 2))
        def _():
            for n in range(2):
                gx_copy(2 * (i - panels // 2) + n).start()

    each(0, panels, main)
    each(chunks, chunks + 2, spreading)
    load_wu.wait()

    @pl.when(col == 1)
    def _():
        moved(hid, (0, own_f), gx_s, gx_r, other_fs).wait_recv()

    strip = min(2 * LANES, width)

    def input_out(n):
        at = pl.ds(pl.multiple_of(n * strip, strip), strip)
        gi_out[:, at] = cols_dot(hid[0, own_ht, :], wu[at, :]).astype(BF16)
    each(0, width // strip, input_out)
    gi_move = remote(gi_out, gi_in, gi_s, gi_r, other_tp)
    gi_move.start()
    each(chunks + 2, chunks + 6, spreading)

    def input_own(n):
        at = pl.ds(pl.multiple_of(n * strip, strip), strip)
        mine = cols_dot(hid[0, own_t, :], wu[at, :]).astype(BF16).astype(F32)
        gi_ref[:, at] = mine.astype(BF16)
    each(0, width // strip, input_own)
    gi_move.wait_recv()
    gi_ref[...] = (gi_ref[...].astype(F32) + gi_in[...].astype(F32)).astype(BF16)
    each(chunks + 6, chunks + take_lag, spreading)

    for move in (y_move(0), y_move(1), cot_move, far_move(0), far_move(1), gi_move):
        move.wait_send()
    some = pl.ds(0, hidden // 2)
    remote(pa_out, pa_in, pa_s, pa_r.at[0], other_fs).wait_send()
    moved(hid, (1 - col, own_f), ya_s, ya_r.at[0], other_y).wait_send()
    moved(hid, (col, own_f), ox_s, act_r.at[0], other_fs).wait_send()
    moved(hid, (col, far_f), fx_s, act_r.at[0], other_fs).wait_send()
    moved(res, (col,), fy_s, fy_r.at[0], other_y).wait_send()

    @pl.when(col == 0)
    def _():
        x_move.wait_send()

    @pl.when(col == 1)
    def _():
        moved(hid, (0, own_f), gx_s, gx_r, other_fs).wait_send()

    @pl.when(middle)
    def _():
        remote(out.at[some], inc.at[1, some], rs_s, rs_r.at[2, 0], inner).wait_send()
        moved(res, (col, some), fc_s, fz_r.at[0, 0], inner).wait_send()

    @pl.when(jnp.logical_not(middle))
    def _():
        remote(out, inc.at[0], rs_s, rs_r.at[0, 0], inner).wait_send()

    @pl.when(has_outer)
    def _():
        moved(res, (col,), fo_s, fz_r.at[0, 0], outer).wait_send()


def scale_kernel(factor, pieces, gi, up, res, gi_out, up_out, down_out, up_wide, down_wide,
                 sems, gi_sem):
    copies = [pltpu.make_async_copy(gi, gi_out, gi_sem)]
    copies[0].start()
    for i in range(pieces):
        for n, (src, wide, dst) in enumerate(
                ((up, up_wide, up_out), (res.at[1], down_wide, down_out))):
            rows = pl.ds(i * (src.shape[0] // pieces), src.shape[0] // pieces)
            wide[rows, :] = src[rows, :].astype(F32) * factor
            copy = pltpu.make_async_copy(wide.at[rows, :], dst.at[rows, :], sems.at[n, i])
            copy.start()
            copies.append(copy)
    for copy in copies:
        copy.wait()


def per_device(n_rep, inputs, pre_act, cotangent, up_weight, down_weight):
    half, width = inputs.shape
    hidden = pre_act.shape[1]
    panels = hidden // LANES
    dma = pltpu.SemaphoreType.DMA
    vmem = pl.BlockSpec(memory_space=pltpu.VMEM)
    anywhere = pl.BlockSpec(memory_space=pl.ANY)
    chunks = 2 * panels
    one = dma((panels,))
    grad_inputs, grad_up, result = pl.pallas_call(
        functools.partial(kernel, n_rep),
        name="ffn_backward",
        out_shape=(
            pltpu.VMEM((half, width), BF16),
            pltpu.VMEM((width, hidden), BF16),
            pltpu.VMEM((2, hidden, width), BF16),
        ),
        in_specs=[anywhere] * 5,
        out_specs=(vmem, vmem, vmem),
        scratch_shapes=[
            pltpu.VMEM((half, hidden), BF16),
            pltpu.VMEM((width, hidden), BF16),
            pltpu.VMEM((hidden, width), BF16),
            pltpu.VMEM((2, 4 * half, width), BF16),
            pltpu.VMEM((2, 4 * half, hidden), BF16),
            pltpu.VMEM((half, hidden), F32),
            pltpu.VMEM((half, hidden), BF16),
            pltpu.VMEM((half, hidden), BF16),
            pltpu.VMEM((half, width), BF16),
            pltpu.VMEM((half, width), BF16),
            pltpu.VMEM((LANES, width // 2), F32),
            pltpu.VMEM((hidden, width), BF16),
            pltpu.VMEM((2, hidden, width), BF16),
            dma((5,)), dma((4,)), dma((4,)), dma((2,)), dma((2,)),
            dma, one, dma, dma, one, dma, dma,
            dma, one, dma, dma,
            dma, dma((3, chunks)), dma, dma, dma((chunks, 2)), dma, dma((chunks,)),
        ],
        compiler_params=pltpu.CompilerParams(
            collective_id=0, has_side_effects=True, vmem_limit_bytes=48 * 2**20
        ),
    )(inputs, pre_act, cotangent, up_weight, down_weight)
    factor = (half * n_rep * lax.axis_size("tp")) ** (-0.5)
    pieces = 8
    return pl.pallas_call(
        functools.partial(scale_kernel, factor, pieces),
        name="scale_outputs",
        out_shape=(
            jax.ShapeDtypeStruct((half, width), BF16),
            jax.ShapeDtypeStruct((width, hidden), F32),
            jax.ShapeDtypeStruct((hidden, width), F32),
        ),
        in_specs=[vmem] * 3,
        out_specs=[anywhere] * 3,
        scratch_shapes=[
            pltpu.VMEM((width, hidden), F32),
            pltpu.VMEM((hidden, width), F32),
            dma((2, pieces)),
            dma,
        ],
        compiler_params=pltpu.CompilerParams(vmem_limit_bytes=40 * 2**20),
    )(*[pltpu.with_memory_space_constraint(g, pltpu.VMEM)
        for g in (grad_inputs, grad_up, result)])


def solution(mesh):
    assert mesh.shape["fs"] == 2 and mesh.shape["tp"] == 2 and mesh.shape["rep"] % 4 == 0
    placed = (
        P(("rep", "tp"), "fs"),
        P(("rep", "fs"), "tp"),
        P(("rep", "tp"), "fs"),
        P("fs", "tp"),
        P("tp", "fs"),
    )
    return jax.shard_map(
        functools.partial(per_device, mesh.shape["rep"]),
        mesh=mesh,
        in_specs=placed,
        out_specs=(P(("rep", "tp"), "fs"), P("fs", "tp"), P("tp", "fs")),
        check_vma=False,
    )
```

```python
import functools

import jax
import jax.numpy as jnp
from jax import lax
from jax.experimental import pallas as pl
from jax.experimental.pallas import tpu as pltpu
from jax.sharding import PartitionSpec as P

MESH = pl.DeviceIdType.MESH
LANES = 128
F32, BF16 = jnp.float32, jnp.bfloat16

START, HOP, PACE = 2, 2, 3
CROSS, SPREAD, APART, TAKE = 1, 3, 4, 6


def rows_dot(left, right):
    return lax.dot_general(left, right, (((0,), (0,)), ((), ())), preferred_element_type=F32)


def cols_dot(left, right):
    return lax.dot_general(left, right, (((1,), (1,)), ((), ())), preferred_element_type=F32)


def kernel(
    n_rep, x_hbm, pre_hbm, cot_hbm, wu_hbm, wd_hbm,
    gi_ref, up_ref, res,
    pre_ref, wu, wd, tok, hid, pa_own, pa_out, pa_in, gi_out, gi_in, part, out, inc,
    w_sem, tp_s, tp_r, yt_s, yt_r, ya_s, ya_r, ox_s, fx_s, act_r, gx_s, gx_r,
    pa_s, pa_r, gi_s, gi_r, rs_s, rs_r, fc_s, fo_s, fz_r, fy_s, fy_r,
):
    half, hidden = pre_ref.shape
    width = wd.shape[1]
    panels = hidden // LANES
    sub, wide = LANES // 2, width // 2
    chunks = 2 * panels
    rep, fs, tp = lax.axis_index("rep"), lax.axis_index("fs"), lax.axis_index("tp")
    rows_n = n_rep // 2
    mid = rows_n // 2
    row, col = rep // 2, rep % 2
    side = jnp.where(row >= mid, 1, 0)
    depth = jnp.where(row >= mid, row - mid, mid - 1 - row)
    has_outer = depth < mid - 1
    middle = depth == 0
    step = 2 * side - 1

    def rep_at(r):
        return 2 * lax.rem(r + rows_n, rows_n) + col

    outer, inner = {"rep": rep_at(row + step)}, {"rep": rep_at(row - step)}
    other_y = {"rep": 2 * row + 1 - col}
    other_fs, other_tp = {"fs": 1 - fs}, {"tp": 1 - tp}

    def block(c, b):
        return pl.ds(pl.multiple_of((2 * c + b) * half, half), half)

    own_f, own_hf = block(col, fs), block(col, 1 - fs)
    far_f, far_hf = block(1 - col, fs), block(1 - col, 1 - fs)
    own_t, own_ht = block(col, tp), block(col, 1 - tp)
    far_t, far_ht = block(1 - col, tp), block(1 - col, 1 - tp)

    def remote(src, dst, s, r, dev):
        return pltpu.make_async_remote_copy(
            src_ref=src, dst_ref=dst, send_sem=s, recv_sem=r, device_id=dev,
            device_id_type=MESH)

    barrier = pltpu.get_barrier_semaphore()
    for dev in (outer, inner, other_y, other_fs, other_tp):
        pl.semaphore_signal(barrier, inc=1, device_id=dev, device_id_type=MESH)
    held = ((cot_hbm, tok.at[1, own_t]), (x_hbm, tok.at[0, own_t]), (pre_hbm, pre_ref),
            (wd_hbm, wd), (wu_hbm, wu))
    loads = [pltpu.make_async_copy(src, dst, w_sem.at[i]) for i, (src, dst) in enumerate(held)]
    load_cot, load_x, load_pre, load_wd, load_wu = loads
    for load in loads:
        load.start()
    load_cot.wait()
    load_x.wait()
    pl.semaphore_wait(barrier, 5)

    def lanes(k):
        return pl.ds(pl.multiple_of(k * LANES, LANES), LANES)

    def where_is(k):
        early = k < 4
        return jnp.where(early, k % 2, k // 2), jnp.where(early, k // 2, k % 2)

    def cols(w):
        return pl.ds(pl.multiple_of(w * wide, wide), wide)

    def piece(k, s):
        p, w = where_is(k)
        return pl.ds(pl.multiple_of(p * LANES + s * sub, sub), sub), cols(w)

    def moved(ref, at, s, r, dev):
        return remote(ref.at[at], ref.at[at], s, r, dev)

    def y_move(w):
        return moved(tok, (1 - col, own_t, cols(w)), yt_s.at[w], yt_r.at[w], other_y)

    def far_move(w):
        return moved(tok, (col, far_t, cols(w)), tp_s.at[2 + w], tp_r.at[2 + w], other_tp)

    y_move(0).start()
    cot_move = moved(tok, (1, own_t), tp_s.at[0], tp_r.at[0], other_tp)
    cot_move.start()
    x_move = moved(tok, (0, own_t), tp_s.at[1], tp_r.at[1], other_tp)

    @pl.when(col == 0)
    def _():
        x_move.start()

    def ya_copy(k):
        return moved(hid, (1 - col, own_f, lanes(k)), ya_s, ya_r.at[k], other_y)

    def ox_copy(k):
        return moved(hid, (col, own_f, lanes(k)), ox_s, act_r.at[k], other_fs)

    def fx_copy(k):
        return moved(hid, (col, far_f, lanes(k)), fx_s, act_r.at[k], other_fs)

    def gx_copy(k):
        return moved(hid, (0, own_f, lanes(k)), gx_s, gx_r, other_fs)

    def pa_copy(k):
        return remote(pa_out.at[:, lanes(k)], pa_in.at[:, lanes(k)], pa_s, pa_r.at[k],
                      other_fs)

    load_pre.wait()

    def each(lo, hi, body):
        def once(k, _):
            body(k)
            return 0
        lax.fori_loop(lo, hi, once, 0)

    def own_square(k):
        positive = jnp.maximum(pre_ref[:, lanes(k)].astype(F32), 0.0)
        hid[1, own_f, lanes(k)] = (positive * positive).astype(BF16)

        @pl.when(col == 0)
        def _():
            ya_copy(k).start()

    each(0, 2, own_square)

    @pl.when(col == 0)
    def _():
        y_move(1).start()
    each(2, panels, own_square)
    load_wd.wait()
    cot_move.wait_recv()

    def act(j):
        at = pl.ds(pl.multiple_of(j * 2 * LANES, 2 * LANES), 2 * LANES)
        pa_out[:, at] = cols_dot(tok[1, own_hf, :], wd[at, :]).astype(BF16)
        for n in range(2):
            pa_copy(2 * j + n).start()
        pa_own[:, at] = cols_dot(tok[1, own_f, :], wd[at, :])

    def pair(k):
        ox_copy(k).start()

    def grad(k):
        pa_copy(k).wait_recv()
        positive = jnp.maximum(pre_ref[:, lanes(k)].astype(F32), 0.0)
        total = pa_own[:, lanes(k)] + pa_in[:, lanes(k)].astype(F32)
        hid[0, own_f, lanes(k)] = (2.0 * positive * total).astype(BF16)

        @pl.when(col == 1)
        def _():
            ya_copy(k).start()

    def hop(k):
        remote(hid.at[1 - col, own_f, lanes(k)], hid.at[col, far_f, lanes(k)], ya_s,
               ya_r.at[k], other_y).wait_recv()
        fx_copy(k).start()

    def rs_copy(k, s):
        slot = jnp.where(middle, 1, 0)
        return remote(out.at[piece(k, s)], inc.at[(slot, *piece(k, s))], rs_s,
                      rs_r.at[jnp.where(middle, 2, s), k], inner)

    def rs_wait(slot, k, s):
        remote(out.at[piece(k, s)], inc.at[(slot, *piece(k, s))], rs_s,
               rs_r.at[2 if slot else s, k], inner).wait_recv()

    def final(k, s, sem, dev):
        return moved(res, (col, *piece(k, s)), sem, fz_r.at[k, s], dev)

    def final_y(k, s):
        return moved(res, (col, *piece(k, s)), fy_s, fy_r.at[k], other_y)

    def arrive(k):
        moved(hid, (col, pl.ds(0, 2 * half), lanes(k)), ox_s, act_r.at[k], other_fs).wait_recv()

    def reduce(k):
        p, w = where_is(k)
        part[...] = rows_dot(hid[col, :, lanes(p)], tok[col, :, cols(w)])
        for s in (1 - side, side):
            at = piece(k, s)
            mine = part[pl.ds(pl.multiple_of(s * sub, sub), sub), :]

            @pl.when(has_outer)
            def _():
                rs_wait(0, k, s)
                out[at] = (mine + inc[(0, *at)].astype(F32)).astype(BF16)

            @pl.when(jnp.logical_not(has_outer))
            def _():
                out[at] = mine.astype(BF16)

            if s is side:
                @pl.when(jnp.logical_not(middle))
                def _():
                    rs_copy(k, s).start()
            else:
                rs_copy(k, s).start()

    def spread(k, s):
        @pl.when(has_outer)
        def _():
            final(k, s, fo_s, outer).start()
        final_y(k, s).start()

    def cross(k):
        @pl.when(middle)
        def _():
            at = piece(k, side)
            rs_wait(1, k, side)
            res[(col, *at)] = (out[at].astype(F32) + inc[(1, *at)].astype(F32)).astype(BF16)
            final(k, side, fc_s, inner).start()
            spread(k, side)

    def forward(k):
        final(k, 1 - side, fc_s, inner).wait_recv()
        spread(k, 1 - side)

    def forward_near(k):
        @pl.when(jnp.logical_not(middle))
        def _():
            final(k, side, fc_s, inner).wait_recv()
            spread(k, side)

    def take(k):
        p, w = where_is(k)
        at = (lanes(p), cols(w))
        moved(res, (1 - col, *at), fy_s, fy_r.at[k], other_y).wait_recv()
        up_ref[cols(w), lanes(p)] = res[(0, *at)].T

    def grads_by(i):
        fast = 2 * START + PACE + PACE * i
        slow = 2 * START + 2 * PACE + i
        return jnp.minimum(panels, jnp.where(
            col == 1, jnp.minimum(fast, slow), 2 * START + i))

    def acts_by(i):
        return jnp.minimum(panels // 2, (grads_by(i + 1) + 2 - col) // 2)

    def when_in(i, end, body):
        @pl.when((i >= 0) & (i < end))
        def _():
            body(i)

    act(0)

    @pl.when(col == 1)
    def _():
        each(0, START, pair)
        act(1)

    def ready(k):
        grad(k)

        @pl.when(col == 0)
        def _():
            pair(k)
    each(0, START, ready)

    @pl.when(col == 1)
    def _():
        y_move(1).start()

    @pl.when(col == 0)
    def _():
        act(1)

    def far_arrived(w):
        remote(tok.at[1 - col, own_t, cols(w)], tok.at[col, far_t, cols(w)], yt_s.at[w],
               yt_r.at[w], other_y).wait_recv()
        far_move(w).start()

    far_arrived(0)

    @pl.when(col == 0)
    def _():
        x_move.wait_recv()

    each(0, HOP, hop)
    far_move(0).wait_recv()

    each(2, acts_by(-1), act)
    each(START, grads_by(-1), grad)

    furthest = SPREAD + APART * (mid - 1)
    take_lag = furthest + TAKE

    def spreading(k):
        when_in(k - SPREAD - APART * depth, chunks, forward)
        when_in(k - CROSS - APART * depth, chunks, forward_near)
        when_in(k - CROSS, chunks, cross)
        when_in(k - take_lag, chunks, take)

    def feed(i):
        when_in(i + HOP, panels, pair)

        @pl.when(col == 1)
        def _():
            when_in(i + HOP, panels, hop)
        each(acts_by(i - 1), acts_by(i), act)
        each(grads_by(i - 1), grads_by(i), grad)

        @pl.when(col == 0)
        def _():
            when_in(i + HOP, panels, hop)

    def main(i):
        @pl.when(has_outer)
        def _():
            feed(i)

        @pl.when(i == 1)
        def _():
            far_arrived(1)
            far_move(1).wait_recv()
        for n in range(2):
            @pl.when(i == 0)
            def _():
                arrive(n)
            if n == 0:
                @pl.when(i > 1)
                def _():
                    arrive(i)
            reduce(2 * i + n)
            spreading(2 * i + n)

            if n == 1:
                @pl.when(jnp.logical_not(has_outer))
                def _():
                    feed(i)

        @pl.when((col == 1) & (i >= panels // 2))
        def _():
            for n in range(2):
                gx_copy(2 * (i - panels // 2) + n).start()

    each(0, panels, main)
    each(chunks, chunks + 2, spreading)
    load_wu.wait()

    @pl.when(col == 1)
    def _():
        moved(hid, (0, own_f), gx_s, gx_r, other_fs).wait_recv()

    strip = min(2 * LANES, width)

    def input_out(n):
        at = pl.ds(pl.multiple_of(n * strip, strip), strip)
        gi_out[:, at] = cols_dot(hid[0, own_ht, :], wu[at, :]).astype(BF16)
    each(0, width // strip, input_out)
    gi_move = remote(gi_out, gi_in, gi_s, gi_r, other_tp)
    gi_move.start()
    each(chunks + 2, chunks + 6, spreading)

    def input_own(n):
        at = pl.ds(pl.multiple_of(n * strip, strip), strip)
        mine = cols_dot(hid[0, own_t, :], wu[at, :]).astype(BF16).astype(F32)
        gi_ref[:, at] = mine.astype(BF16)
    each(0, width // strip, input_own)
    gi_move.wait_recv()
    gi_ref[...] = (gi_ref[...].astype(F32) + gi_in[...].astype(F32)).astype(BF16)
    each(chunks + 6, chunks + take_lag, spreading)

    for move in (y_move(0), y_move(1), cot_move, far_move(0), far_move(1), gi_move):
        move.wait_send()
    some = pl.ds(0, hidden // 2)
    remote(pa_out, pa_in, pa_s, pa_r.at[0], other_fs).wait_send()
    moved(hid, (1 - col, own_f), ya_s, ya_r.at[0], other_y).wait_send()
    moved(hid, (col, own_f), ox_s, act_r.at[0], other_fs).wait_send()
    moved(hid, (col, far_f), fx_s, act_r.at[0], other_fs).wait_send()
    moved(res, (col,), fy_s, fy_r.at[0], other_y).wait_send()

    @pl.when(col == 0)
    def _():
        x_move.wait_send()

    @pl.when(col == 1)
    def _():
        moved(hid, (0, own_f), gx_s, gx_r, other_fs).wait_send()

    @pl.when(middle)
    def _():
        remote(out.at[some], inc.at[1, some], rs_s, rs_r.at[2, 0], inner).wait_send()
        moved(res, (col, some), fc_s, fz_r.at[0, 0], inner).wait_send()

    @pl.when(jnp.logical_not(middle))
    def _():
        remote(out, inc.at[0], rs_s, rs_r.at[0, 0], inner).wait_send()

    @pl.when(has_outer)
    def _():
        moved(res, (col,), fo_s, fz_r.at[0, 0], outer).wait_send()


def scale_kernel(factor, pieces, gi, up, res, gi_out, up_out, down_out, up_wide, down_wide,
                 sems, gi_sem):
    copies = [pltpu.make_async_copy(gi, gi_out, gi_sem)]
    copies[0].start()
    for i in range(pieces):
        for n, (src, wide, dst) in enumerate(
                ((up, up_wide, up_out), (res.at[1], down_wide, down_out))):
            rows = pl.ds(i * (src.shape[0] // pieces), src.shape[0] // pieces)
            wide[rows, :] = src[rows, :].astype(F32) * factor
            copy = pltpu.make_async_copy(wide.at[rows, :], dst.at[rows, :], sems.at[n, i])
            copy.start()
            copies.append(copy)
    for copy in copies:
        copy.wait()


def per_device(n_rep, inputs, pre_act, cotangent, up_weight, down_weight):
    half, width = inputs.shape
    hidden = pre_act.shape[1]
    panels = hidden // LANES
    dma = pltpu.SemaphoreType.DMA
    vmem = pl.BlockSpec(memory_space=pltpu.VMEM)
    anywhere = pl.BlockSpec(memory_space=pl.ANY)
    chunks = 2 * panels
    one = dma((panels,))
    grad_inputs, grad_up, result = pl.pallas_call(
        functools.partial(kernel, n_rep),
        name="ffn_backward",
        out_shape=(
            pltpu.VMEM((half, width), BF16),
            pltpu.VMEM((width, hidden), BF16),
            pltpu.VMEM((2, hidden, width), BF16),
        ),
        in_specs=[anywhere] * 5,
        out_specs=(vmem, vmem, vmem),
        scratch_shapes=[
            pltpu.VMEM((half, hidden), BF16),
            pltpu.VMEM((width, hidden), BF16),
            pltpu.VMEM((hidden, width), BF16),
            pltpu.VMEM((2, 4 * half, width), BF16),
            pltpu.VMEM((2, 4 * half, hidden), BF16),
            pltpu.VMEM((half, hidden), F32),
            pltpu.VMEM((half, hidden), BF16),
            pltpu.VMEM((half, hidden), BF16),
            pltpu.VMEM((half, width), BF16),
            pltpu.VMEM((half, width), BF16),
            pltpu.VMEM((LANES, width // 2), F32),
            pltpu.VMEM((hidden, width), BF16),
            pltpu.VMEM((2, hidden, width), BF16),
            dma((5,)), dma((4,)), dma((4,)), dma((2,)), dma((2,)),
            dma, one, dma, dma, one, dma, dma,
            dma, one, dma, dma,
            dma, dma((3, chunks)), dma, dma, dma((chunks, 2)), dma, dma((chunks,)),
        ],
        compiler_params=pltpu.CompilerParams(
            collective_id=0, has_side_effects=True, vmem_limit_bytes=48 * 2**20
        ),
    )(inputs, pre_act, cotangent, up_weight, down_weight)
    factor = (half * n_rep * lax.axis_size("tp")) ** (-0.5)
    pieces = 8
    return pl.pallas_call(
        functools.partial(scale_kernel, factor, pieces),
        name="scale_outputs",
        out_shape=(
            jax.ShapeDtypeStruct((half, width), BF16),
            jax.ShapeDtypeStruct((width, hidden), F32),
            jax.ShapeDtypeStruct((hidden, width), F32),
        ),
        in_specs=[vmem] * 3,
        out_specs=[anywhere] * 3,
        scratch_shapes=[
            pltpu.VMEM((width, hidden), F32),
            pltpu.VMEM((hidden, width), F32),
            dma((2, pieces)),
            dma,
        ],
        compiler_params=pltpu.CompilerParams(vmem_limit_bytes=40 * 2**20),
    )(*[pltpu.with_memory_space_constraint(g, pltpu.VMEM)
        for g in (grad_inputs, grad_up, result)])


def solution(mesh):
    assert mesh.shape["fs"] == 2 and mesh.shape["tp"] == 2 and mesh.shape["rep"] % 4 == 0
    placed = (
        P(("rep", "tp"), "fs"),
        P(("rep", "fs"), "tp"),
        P(("rep", "tp"), "fs"),
        P("fs", "tp"),
        P("tp", "fs"),
    )
    return jax.shard_map(
        functools.partial(per_device, mesh.shape["rep"]),
        mesh=mesh,
        in_specs=placed,
        out_specs=(P(("rep", "tp"), "fs"), P("fs", "tp"), P("tp", "fs")),
        check_vma=False,
    )
```

```python
import functools

import jax
import jax.numpy as jnp
from jax import lax
from jax.experimental import pallas as pl
from jax.experimental.pallas import tpu as pltpu
from jax.sharding import PartitionSpec as P

MESH = pl.DeviceIdType.MESH
LANES = 128
F32, BF16 = jnp.float32, jnp.bfloat16

START, HOP, PACE = 2, 2, 3
CROSS, SPREAD, APART, TAKE = 1, 3, 4, 6
RELAY, LATE = 16, 9


def rows_dot(left, right):
    return lax.dot_general(left, right, (((0,), (0,)), ((), ())), preferred_element_type=F32)


def cols_dot(left, right):
    return lax.dot_general(left, right, (((1,), (1,)), ((), ())), preferred_element_type=F32)


def kernel(
    n_rep, x_hbm, pre_hbm, cot_hbm, wu_hbm, wd_hbm,
    gi_ref, up_ref, res,
    pre_ref, wu, wd, tok, hid, pa_own, pa_out, pa_in, gi_out, gi_in, part, out, inc,
    w_sem, tp_s, tp_r, yt_s, yt_r, ya_s, ya_r, ox_s, fx_s, act_r, gx_s, gx_r,
    pa_s, pa_r, gi_s, gi_r, rs_s, rs_r, fc_s, fo_s, fz_r, fy_s, fy_r, rc_s, ro_s, rz_r,
):
    half, hidden = pre_ref.shape
    width = wd.shape[1]
    panels = hidden // LANES
    sub, wide = LANES // 2, width // 2
    chunks = 2 * panels
    rep, fs, tp = lax.axis_index("rep"), lax.axis_index("fs"), lax.axis_index("tp")
    rows_n = n_rep // 2
    mid = rows_n // 2
    row, col = rep // 2, rep % 2
    side = jnp.where(row >= mid, 1, 0)
    depth = jnp.where(row >= mid, row - mid, mid - 1 - row)
    has_outer = depth < mid - 1
    middle = depth == 0
    step = 2 * side - 1

    def rep_at(r):
        return 2 * lax.rem(r + rows_n, rows_n) + col

    outer, inner = {"rep": rep_at(row + step)}, {"rep": rep_at(row - step)}
    other_y = {"rep": 2 * row + 1 - col}
    other_fs, other_tp = {"fs": 1 - fs}, {"tp": 1 - tp}

    def block(c, b):
        return pl.ds(pl.multiple_of((2 * c + b) * half, half), half)

    own_f, own_hf = block(col, fs), block(col, 1 - fs)
    far_f, far_hf = block(1 - col, fs), block(1 - col, 1 - fs)
    own_t, own_ht = block(col, tp), block(col, 1 - tp)
    far_t, far_ht = block(1 - col, tp), block(1 - col, 1 - tp)

    def remote(src, dst, s, r, dev):
        return pltpu.make_async_remote_copy(
            src_ref=src, dst_ref=dst, send_sem=s, recv_sem=r, device_id=dev,
            device_id_type=MESH)

    barrier = pltpu.get_barrier_semaphore()
    for dev in (outer, inner, other_y, other_fs, other_tp):
        pl.semaphore_signal(barrier, inc=1, device_id=dev, device_id_type=MESH)
    first = pl.ds(0, 2 * LANES)
    rest = pl.ds(2 * LANES, hidden - 2 * LANES)
    held = ((cot_hbm, tok.at[1, own_t]), (x_hbm, tok.at[0, own_t]), (pre_hbm, pre_ref),
            (wd_hbm.at[first], wd.at[first]), (wd_hbm.at[rest], wd.at[rest]), (wu_hbm, wu))
    loads = [pltpu.make_async_copy(src, dst, w_sem.at[i]) for i, (src, dst) in enumerate(held)]
    load_cot, load_x, load_pre, load_first, load_rest, load_wu = loads
    for load in loads[:4]:
        load.start()
    load_cot.wait()
    load_x.wait()
    pl.semaphore_wait(barrier, 5)

    def lanes(k):
        return pl.ds(pl.multiple_of(k * LANES, LANES), LANES)

    def where_is(k):
        early = k < 4
        return jnp.where(early, k % 2, k // 2), jnp.where(early, k // 2, k % 2)

    def cols(w):
        return pl.ds(pl.multiple_of(w * wide, wide), wide)

    def piece(k, s):
        p, w = where_is(k)
        return pl.ds(pl.multiple_of(p * LANES + s * sub, sub), sub), cols(w)

    def moved(ref, at, s, r, dev):
        return remote(ref.at[at], ref.at[at], s, r, dev)

    def y_move(w):
        return moved(tok, (1 - col, own_t, cols(w)), yt_s.at[w], yt_r.at[w], other_y)

    def far_move(w):
        return moved(tok, (col, far_t, cols(w)), tp_s.at[2 + w], tp_r.at[2 + w], other_tp)

    y_move(0).start()
    cot_move = moved(tok, (1, own_t), tp_s.at[0], tp_r.at[0], other_tp)
    cot_move.start()
    x_move = moved(tok, (0, own_t), tp_s.at[1], tp_r.at[1], other_tp)

    @pl.when(col == 0)
    def _():
        x_move.start()

    def ya_copy(k):
        return moved(hid, (1 - col, own_f, lanes(k)), ya_s, ya_r.at[k], other_y)

    def ox_copy(k):
        return moved(hid, (col, own_f, lanes(k)), ox_s, act_r.at[k], other_fs)

    def fx_copy(k):
        return moved(hid, (col, far_f, lanes(k)), fx_s, act_r.at[k], other_fs)

    def gx_copy(k):
        return moved(hid, (0, own_f, lanes(k)), gx_s, gx_r, other_fs)

    def pa_copy(k):
        return remote(pa_out.at[:, lanes(k)], pa_in.at[:, lanes(k)], pa_s, pa_r.at[k],
                      other_fs)

    load_pre.wait()

    def each(lo, hi, body):
        def once(k, _):
            body(k)
            return 0
        lax.fori_loop(lo, hi, once, 0)

    def own_square(k):
        positive = jnp.maximum(pre_ref[:, lanes(k)].astype(F32), 0.0)
        hid[1, own_f, lanes(k)] = (positive * positive).astype(BF16)

        @pl.when(col == 0)
        def _():
            ya_copy(k).start()

    each(0, 2, own_square)

    @pl.when(col == 0)
    def _():
        y_move(1).start()
    load_rest.start()
    load_wu.start()
    load_first.wait()
    cot_move.wait_recv()

    def act(j):
        at = pl.ds(pl.multiple_of(j * 2 * LANES, 2 * LANES), 2 * LANES)
        pa_out[:, at] = cols_dot(tok[1, own_hf, :], wd[at, :]).astype(BF16)
        for n in range(2):
            pa_copy(2 * j + n).start()
        pa_own[:, at] = cols_dot(tok[1, own_f, :], wd[at, :])

    def pair(k):
        ox_copy(k).start()

    def grad(k):
        pa_copy(k).wait_recv()
        positive = jnp.maximum(pre_ref[:, lanes(k)].astype(F32), 0.0)
        total = pa_own[:, lanes(k)] + pa_in[:, lanes(k)].astype(F32)
        hid[0, own_f, lanes(k)] = (2.0 * positive * total).astype(BF16)

        @pl.when(col == 1)
        def _():
            ya_copy(k).start()

    def hop(k):
        remote(hid.at[1 - col, own_f, lanes(k)], hid.at[col, far_f, lanes(k)], ya_s,
               ya_r.at[k], other_y).wait_recv()
        fx_copy(k).start()

    def rs_copy(k, s):
        slot = jnp.where(middle, 1, 0)
        return remote(out.at[piece(k, s)], inc.at[(slot, *piece(k, s))], rs_s,
                      rs_r.at[jnp.where(middle, 2, s), k], inner)

    def rs_wait(slot, k, s):
        remote(out.at[piece(k, s)], inc.at[(slot, *piece(k, s))], rs_s,
               rs_r.at[2 if slot else s, k], inner).wait_recv()

    def final(k, s, sem, dev):
        return moved(res, (col, *piece(k, s)), sem, fz_r.at[k, s], dev)

    def final_y(k, s):
        return moved(res, (col, *piece(k, s)), fy_s, fy_r.at[k], other_y)

    def arrive(k):
        moved(hid, (col, pl.ds(0, 2 * half), lanes(k)), ox_s, act_r.at[k], other_fs).wait_recv()

    def reduce(k):
        p, w = where_is(k)
        part[...] = rows_dot(hid[col, :, lanes(p)], tok[col, :, cols(w)])
        for s in (1 - side, side):
            at = piece(k, s)
            mine = part[pl.ds(pl.multiple_of(s * sub, sub), sub), :]

            @pl.when(has_outer)
            def _():
                rs_wait(0, k, s)
                out[at] = (mine + inc[(0, *at)].astype(F32)).astype(BF16)

            @pl.when(jnp.logical_not(has_outer))
            def _():
                out[at] = mine.astype(BF16)

            if s is side:
                @pl.when(jnp.logical_not(middle))
                def _():
                    rs_copy(k, s).start()
            else:
                rs_copy(k, s).start()

    def relayed(k):
        return k % RELAY == RELAY // 2

    def spread(k, s):
        @pl.when(has_outer)
        def _():
            final(k, s, fo_s, outer).start()

    def spread_y(k, s):
        spread(k, s)

        @pl.when(jnp.logical_not(relayed(k)))
        def _():
            final_y(k, s).start()

    def cross(k):
        @pl.when(middle)
        def _():
            at = piece(k, side)
            rs_wait(1, k, side)
            res[(col, *at)] = (out[at].astype(F32) + inc[(1, *at)].astype(F32)).astype(BF16)
            final(k, side, fc_s, inner).start()
            spread(k, side)
            final_y(k, side).start()

    def forward(k):
        final(k, 1 - side, fc_s, inner).wait_recv()
        spread_y(k, 1 - side)

    def forward_near(k):
        @pl.when(jnp.logical_not(middle))
        def _():
            final(k, side, fc_s, inner).wait_recv()
            spread_y(k, side)

    def relay(k, s, sem, dev):
        return moved(res, (1 - col, *piece(k, s)), sem, rz_r.at[k // RELAY, s], dev)

    def relay_out(k, s):
        @pl.when(has_outer)
        def _():
            relay(k, s, ro_s, outer).start()

    def relay_near(k):
        @pl.when(relayed(k))
        def _():
            @pl.when(middle)
            def _():
                moved(res, (1 - col, *piece(k, side)), fy_s, fy_r.at[k], other_y).wait_recv()
                relay(k, side, rc_s, inner).start()

            @pl.when(jnp.logical_not(middle))
            def _():
                relay(k, side, rc_s, inner).wait_recv()
            relay_out(k, side)

    def relay_far(k):
        @pl.when(relayed(k))
        def _():
            relay(k, 1 - side, rc_s, inner).wait_recv()
            relay_out(k, 1 - side)

    def take(k):
        p, w = where_is(k)
        at = (lanes(p), cols(w))

        @pl.when(jnp.logical_not(relayed(k)))
        def _():
            moved(res, (1 - col, *at), fy_s, fy_r.at[k], other_y).wait_recv()
        up_ref[cols(w), lanes(p)] = res[(0, *at)].T

    def grads_by(i):
        fast = 2 * START + PACE + PACE * i
        slow = 2 * START + 2 * PACE + i
        return jnp.minimum(panels, jnp.where(
            col == 1, jnp.minimum(fast, slow), START + 1 + i))

    def acts_by(i):
        return jnp.minimum(panels // 2, (grads_by(i + 1) + 2 - col) // 2)

    def when_in(i, end, body):
        @pl.when((i >= 0) & (i < end))
        def _():
            body(i)

    act(0)
    each(2, panels, own_square)
    load_rest.wait()

    @pl.when(col == 1)
    def _():
        each(0, START, pair)
        act(1)

    def ready(k):
        grad(k)

        @pl.when(col == 0)
        def _():
            pair(k)
    each(0, START, ready)

    @pl.when(col == 1)
    def _():
        y_move(1).start()

    def far_arrived(w):
        remote(tok.at[1 - col, own_t, cols(w)], tok.at[col, far_t, cols(w)], yt_s.at[w],
               yt_r.at[w], other_y).wait_recv()
        far_move(w).start()

    far_arrived(0)

    @pl.when(col == 0)
    def _():
        x_move.wait_recv()

    each(0, HOP, hop)
    far_move(0).wait_recv()

    each(2 - jnp.where(col == 0, 1, 0), acts_by(-1), act)
    each(START, grads_by(-1), grad)

    furthest = SPREAD + APART * (mid - 1)
    take_lag = furthest + max(TAKE, LATE + 2 * CROSS + 1 - SPREAD)

    def spreading(k):
        when_in(k - SPREAD - APART * depth, chunks, forward)
        when_in(k - CROSS - APART * depth, chunks, forward_near)
        when_in(k - CROSS, chunks, cross)
        when_in(k - LATE - APART * depth, chunks, relay_near)
        when_in(k - LATE - 2 * CROSS - APART * depth, chunks, relay_far)
        when_in(k - take_lag, chunks, take)

    def feed(i):
        @pl.when(col == 1)
        def _():
            when_in(i + HOP, panels, pair)
            when_in(i + HOP, panels, hop)
        each(acts_by(i - 1), acts_by(i), act)

        @pl.when(i == 0)
        def _():
            far_arrived(1)
        each(grads_by(i - 1), grads_by(i), grad)

        @pl.when(col == 0)
        def _():
            when_in(i + HOP, panels, pair)
            when_in(i + HOP, panels, hop)

    def main(i):
        @pl.when(has_outer)
        def _():
            feed(i)

        @pl.when(i == 1)
        def _():
            far_move(1).wait_recv()
        for n in range(2):
            @pl.when(i == 0)
            def _():
                arrive(n)
            if n == 0:
                @pl.when(i > 1)
                def _():
                    arrive(i)
            reduce(2 * i + n)
            spreading(2 * i + n)

            if n == 1:
                @pl.when(jnp.logical_not(has_outer))
                def _():
                    feed(i)

        @pl.when((col == 1) & (i >= panels // 2))
        def _():
            for n in range(2):
                gx_copy(2 * (i - panels // 2) + n).start()

    each(0, panels, main)
    load_wu.wait()
    strip = min(2 * LANES, width)

    def input_out(n):
        at = pl.ds(pl.multiple_of(n * strip, strip), strip)
        gi_out[:, at] = cols_dot(hid[0, own_ht, :], wu[at, :]).astype(BF16)
    def input_own(n):
        at = pl.ds(pl.multiple_of(n * strip, strip), strip)
        mine = cols_dot(hid[0, own_t, :], wu[at, :]).astype(BF16).astype(F32)
        gi_ref[:, at] = mine.astype(BF16)
    strips = width // strip
    gi_move = remote(gi_out, gi_in, gi_s, gi_r, other_tp)

    def finish(n):
        spreading(chunks + n)
        m = n - jnp.where(has_outer, SPREAD, 0)

        @pl.when((col == 1) & (m == 0))
        def _():
            moved(hid, (0, own_f), gx_s, gx_r, other_fs).wait_recv()

        for h in range(2):
            when_in(2 * m + h, strips, input_out)
        for h in range(2):
            when_in(2 * m + h - strips, strips, input_own)

        @pl.when(m == strips // 2 - 1)
        def _():
            gi_move.start()
    each(0, SPREAD + strips, finish)
    each(chunks + SPREAD + strips, chunks + take_lag, spreading)
    gi_move.wait_recv()
    gi_ref[...] = (gi_ref[...].astype(F32) + gi_in[...].astype(F32)).astype(BF16)

    for move in (y_move(0), y_move(1), cot_move, far_move(0), far_move(1), gi_move):
        move.wait_send()
    some = pl.ds(0, hidden // 2)
    remote(pa_out, pa_in, pa_s, pa_r.at[0], other_fs).wait_send()
    moved(hid, (1 - col, own_f), ya_s, ya_r.at[0], other_y).wait_send()
    moved(hid, (col, own_f), ox_s, act_r.at[0], other_fs).wait_send()
    moved(hid, (col, far_f), fx_s, act_r.at[0], other_fs).wait_send()
    relays = len(range(RELAY // 2, chunks, RELAY))
    passed = relays * sub // 2

    @pl.when(col == 0)
    def _():
        x_move.wait_send()

    @pl.when(col == 1)
    def _():
        moved(hid, (0, own_f), gx_s, gx_r, other_fs).wait_send()

    @pl.when(middle)
    def _():
        remote(out.at[some], inc.at[1, some], rs_s, rs_r.at[2, 0], inner).wait_send()
        moved(res, (col, some), fc_s, fz_r.at[0, 0], inner).wait_send()
        kept = pl.ds(0, hidden - passed)
        moved(res, (col, kept), fy_s, fy_r.at[0], other_y).wait_send()
        moved(res, (1 - col, pl.ds(0, passed)), rc_s, rz_r.at[0, 0], inner).wait_send()

    @pl.when(jnp.logical_not(middle))
    def _():
        remote(out, inc.at[0], rs_s, rs_r.at[0, 0], inner).wait_send()
        kept = pl.ds(0, hidden - 2 * passed)
        moved(res, (col, kept), fy_s, fy_r.at[0], other_y).wait_send()

    @pl.when(has_outer)
    def _():
        moved(res, (col,), fo_s, fz_r.at[0, 0], outer).wait_send()
        moved(res, (1 - col, pl.ds(0, 2 * passed)), ro_s, rz_r.at[0, 0], outer).wait_send()


def scale_kernel(factor, pieces, gi, up, res, gi_out, up_out, down_out, up_wide, down_wide,
                 sems, gi_sem):
    copies = [pltpu.make_async_copy(gi, gi_out, gi_sem)]
    copies[0].start()
    for i in range(pieces):
        for n, (src, wide, dst) in enumerate(
                ((up, up_wide, up_out), (res.at[1], down_wide, down_out))):
            rows = pl.ds(i * (src.shape[0] // pieces), src.shape[0] // pieces)
            wide[rows, :] = src[rows, :].astype(F32) * factor
            copy = pltpu.make_async_copy(wide.at[rows, :], dst.at[rows, :], sems.at[n, i])
            copy.start()
            copies.append(copy)
    for copy in copies:
        copy.wait()


def per_device(n_rep, inputs, pre_act, cotangent, up_weight, down_weight):
    half, width = inputs.shape
    hidden = pre_act.shape[1]
    panels = hidden // LANES
    dma = pltpu.SemaphoreType.DMA
    vmem = pl.BlockSpec(memory_space=pltpu.VMEM)
    anywhere = pl.BlockSpec(memory_space=pl.ANY)
    chunks = 2 * panels
    one = dma((panels,))
    grad_inputs, grad_up, result = pl.pallas_call(
        functools.partial(kernel, n_rep),
        name="ffn_backward",
        out_shape=(
            pltpu.VMEM((half, width), BF16),
            pltpu.VMEM((width, hidden), BF16),
            pltpu.VMEM((2, hidden, width), BF16),
        ),
        in_specs=[anywhere] * 5,
        out_specs=(vmem, vmem, vmem),
        scratch_shapes=[
            pltpu.VMEM((half, hidden), BF16),
            pltpu.VMEM((width, hidden), BF16),
            pltpu.VMEM((hidden, width), BF16),
            pltpu.VMEM((2, 4 * half, width), BF16),
            pltpu.VMEM((2, 4 * half, hidden), BF16),
            pltpu.VMEM((half, hidden), F32),
            pltpu.VMEM((half, hidden), BF16),
            pltpu.VMEM((half, hidden), BF16),
            pltpu.VMEM((half, width), BF16),
            pltpu.VMEM((half, width), BF16),
            pltpu.VMEM((LANES, width // 2), F32),
            pltpu.VMEM((hidden, width), BF16),
            pltpu.VMEM((2, hidden, width), BF16),
            dma((6,)), dma((4,)), dma((4,)), dma((2,)), dma((2,)),
            dma, one, dma, dma, one, dma, dma,
            dma, one, dma, dma,
            dma, dma((3, chunks)), dma, dma, dma((chunks, 2)), dma, dma((chunks,)),
            dma, dma, dma((-(-chunks // RELAY), 2)),
        ],
        compiler_params=pltpu.CompilerParams(
            collective_id=0, has_side_effects=True, vmem_limit_bytes=48 * 2**20
        ),
    )(inputs, pre_act, cotangent, up_weight, down_weight)
    factor = (half * n_rep * lax.axis_size("tp")) ** (-0.5)
    pieces = 8
    return pl.pallas_call(
        functools.partial(scale_kernel, factor, pieces),
        name="scale_outputs",
        out_shape=(
            jax.ShapeDtypeStruct((half, width), BF16),
            jax.ShapeDtypeStruct((width, hidden), F32),
            jax.ShapeDtypeStruct((hidden, width), F32),
        ),
        in_specs=[vmem] * 3,
        out_specs=[anywhere] * 3,
        scratch_shapes=[
            pltpu.VMEM((width, hidden), F32),
            pltpu.VMEM((hidden, width), F32),
            dma((2, pieces)),
            dma,
        ],
        compiler_params=pltpu.CompilerParams(vmem_limit_bytes=40 * 2**20),
    )(*[pltpu.with_memory_space_constraint(g, pltpu.VMEM)
        for g in (grad_inputs, grad_up, result)])


def solution(mesh):
    assert mesh.shape["fs"] == 2 and mesh.shape["tp"] == 2 and mesh.shape["rep"] % 4 == 0
    placed = (
        P(("rep", "tp"), "fs"),
        P(("rep", "fs"), "tp"),
        P(("rep", "tp"), "fs"),
        P("fs", "tp"),
        P("tp", "fs"),
    )
    return jax.shard_map(
        functools.partial(per_device, mesh.shape["rep"]),
        mesh=mesh,
        in_specs=placed,
        out_specs=(P(("rep", "tp"), "fs"), P("fs", "tp"), P("tp", "fs")),
        check_vma=False,
    )
```

```python
import functools

import jax
import jax.numpy as jnp
from jax import lax
from jax.experimental import pallas as pl
from jax.experimental.pallas import tpu as pltpu
from jax.sharding import PartitionSpec as P

MESH = pl.DeviceIdType.MESH
LANES = 128
F32, BF16 = jnp.float32, jnp.bfloat16

START, HOP, PACE = 2, 2, 3
CROSS, SPREAD, APART, TAKE = 1, 3, 4, 6
RELAY, LATE = (32, 16), 9


def rows_dot(left, right):
    return lax.dot_general(left, right, (((0,), (0,)), ((), ())), preferred_element_type=F32)


def cols_dot(left, right):
    return lax.dot_general(left, right, (((1,), (1,)), ((), ())), preferred_element_type=F32)


def turn_of(n_rep, chunks):
    furthest = SPREAD + APART * (n_rep // 4 - 1)
    return min(chunks, 1 << (furthest + TAKE).bit_length())


def kernel(
    n_rep, x_hbm, pre_hbm, cot_hbm, wu_hbm, wd_hbm,
    gi_ref, up_ref, res,
    pre_ref, wu, wd, tok, hid, pa_own, pa_out, pa_in, gi_out, gi_in, part, out, inc,
    w_sem, tp_s, tp_r, yt_s, yt_r, ya_s, ya_r, ox_s, fx_s, act_r, gx_s, gx_r,
    pa_s, pa_r, gi_s, gi_r, rs_s, rs_r, fc_s, fo_s, fz_r, fy_s, fy_r, rc_s, ro_s, rz_r,
):
    half, hidden = pre_ref.shape
    width = wd.shape[1]
    panels = hidden // LANES
    sub, wide = LANES // 2, width // 2
    chunks = 2 * panels
    rep, fs, tp = lax.axis_index("rep"), lax.axis_index("fs"), lax.axis_index("tp")
    rows_n = n_rep // 2
    mid = rows_n // 2
    row, col = rep // 2, rep % 2
    side = jnp.where(row >= mid, 1, 0)
    depth = jnp.where(row >= mid, row - mid, mid - 1 - row)
    has_outer = depth < mid - 1
    middle = depth == 0
    step = 2 * side - 1

    def rep_at(r):
        return 2 * lax.rem(r + rows_n, rows_n) + col

    outer, inner = {"rep": rep_at(row + step)}, {"rep": rep_at(row - step)}
    other_y = {"rep": 2 * row + 1 - col}
    other_fs, other_tp = {"fs": 1 - fs}, {"tp": 1 - tp}

    def block(c, b):
        return pl.ds(pl.multiple_of((2 * c + b) * half, half), half)

    own_f, own_hf = block(col, fs), block(col, 1 - fs)
    far_f, far_hf = block(1 - col, fs), block(1 - col, 1 - fs)
    own_t, own_ht = block(col, tp), block(col, 1 - tp)
    far_t, far_ht = block(1 - col, tp), block(1 - col, 1 - tp)

    def remote(src, dst, s, r, dev):
        return pltpu.make_async_remote_copy(
            src_ref=src, dst_ref=dst, send_sem=s, recv_sem=r, device_id=dev,
            device_id_type=MESH)

    barrier = pltpu.get_barrier_semaphore()
    for dev in (outer, inner, other_y, other_fs, other_tp):
        pl.semaphore_signal(barrier, inc=1, device_id=dev, device_id_type=MESH)
    first = pl.ds(0, 2 * LANES)
    rest = pl.ds(2 * LANES, hidden - 2 * LANES)
    held = ((cot_hbm, tok.at[1, own_t]), (x_hbm, tok.at[0, own_t]), (pre_hbm, pre_ref),
            (wd_hbm.at[first], wd.at[first]), (wd_hbm.at[rest], wd.at[rest]), (wu_hbm, wu))
    loads = [pltpu.make_async_copy(src, dst, w_sem.at[i]) for i, (src, dst) in enumerate(held)]
    load_cot, load_x, load_pre, load_first, load_rest, load_wu = loads
    for load in loads[:4]:
        load.start()
    load_cot.wait()
    load_x.wait()
    pl.semaphore_wait(barrier, 5)

    def lanes(k):
        return pl.ds(pl.multiple_of(k * LANES, LANES), LANES)

    def where_is(k):
        early = k < 4
        return jnp.where(early, k % 2, k // 2), jnp.where(early, k // 2, k % 2)

    def cols(w):
        return pl.ds(pl.multiple_of(w * wide, wide), wide)

    def piece(k, s):
        p, w = where_is(k)
        return pl.ds(pl.multiple_of(p * LANES + s * sub, sub), sub), cols(w)

    turn = turn_of(n_rep, chunks)

    def moved(ref, at, s, r, dev):
        return remote(ref.at[at], ref.at[at], s, r, dev)

    def y_move(w):
        return moved(tok, (1 - col, own_t, cols(w)), yt_s.at[w], yt_r.at[w], other_y)

    def far_move(w):
        return moved(tok, (col, far_t, cols(w)), tp_s.at[2 + w], tp_r.at[2 + w], other_tp)

    y_move(0).start()
    cot_move = moved(tok, (1, own_t), tp_s.at[0], tp_r.at[0], other_tp)
    cot_move.start()
    x_move = moved(tok, (0, own_t), tp_s.at[1], tp_r.at[1], other_tp)

    @pl.when(col == 0)
    def _():
        x_move.start()

    def ya_copy(k):
        return moved(hid, (1 - col, own_f, lanes(k)), ya_s, ya_r.at[k], other_y)

    def ox_copy(k):
        return moved(hid, (col, own_f, lanes(k)), ox_s, act_r.at[k], other_fs)

    def fx_copy(k):
        return moved(hid, (col, far_f, lanes(k)), fx_s, act_r.at[k], other_fs)

    def gx_copy(k):
        return moved(hid, (0, own_f, lanes(k)), gx_s, gx_r, other_fs)

    def pa_copy(k):
        return remote(pa_out.at[:, lanes(k)], pa_in.at[:, lanes(k)], pa_s, pa_r.at[k],
                      other_fs)

    load_pre.wait()

    def each(lo, hi, body):
        def once(k, _):
            body(k)
            return 0
        lax.fori_loop(lo, hi, once, 0)

    def own_square(k):
        positive = jnp.maximum(pre_ref[:, lanes(k)].astype(F32), 0.0)
        hid[1, own_f, lanes(k)] = (positive * positive).astype(BF16)

        @pl.when(col == 0)
        def _():
            ya_copy(k).start()

    each(0, 2, own_square)

    @pl.when(col == 0)
    def _():
        y_move(1).start()
    load_rest.start()
    load_wu.start()
    load_first.wait()
    cot_move.wait_recv()

    def act(j):
        at = pl.ds(pl.multiple_of(j * 2 * LANES, 2 * LANES), 2 * LANES)
        pa_out[:, at] = cols_dot(tok[1, own_hf, :], wd[at, :]).astype(BF16)
        for n in range(2):
            pa_copy(2 * j + n).start()
        pa_own[:, at] = cols_dot(tok[1, own_f, :], wd[at, :])

    def pair(k):
        ox_copy(k).start()

    def grad(k):
        pa_copy(k).wait_recv()
        positive = jnp.maximum(pre_ref[:, lanes(k)].astype(F32), 0.0)
        total = pa_own[:, lanes(k)] + pa_in[:, lanes(k)].astype(F32)
        hid[0, own_f, lanes(k)] = (2.0 * positive * total).astype(BF16)

        @pl.when(col == 1)
        def _():
            ya_copy(k).start()

    def hop(k):
        remote(hid.at[1 - col, own_f, lanes(k)], hid.at[col, far_f, lanes(k)], ya_s,
               ya_r.at[k], other_y).wait_recv()
        fx_copy(k).start()

    def rs_copy(k, s, recv):
        slot = jnp.where(middle, 1, 0)
        return remote(out.at[piece(k, s)], inc.at[(slot, *piece(k, s))], rs_s,
                      recv.at[k % turn, s], inner)

    def rs_start(k, s):
        @pl.when(middle)
        def _():
            rs_copy(k, s, fz_r).start()

        @pl.when(jnp.logical_not(middle))
        def _():
            rs_copy(k, s, rs_r).start()

    def final(k, s, sem, dev):
        return moved(res, (col, *piece(k, s)), sem, fz_r.at[k % turn, s], dev)

    def final_y(k, s):
        return moved(res, (col, *piece(k, s)), fy_s, fy_r.at[k], other_y)

    def arrive(k):
        moved(hid, (col, pl.ds(0, 2 * half), lanes(k)), ox_s, act_r.at[k], other_fs).wait_recv()

    def reduce(k):
        p, w = where_is(k)
        part[...] = rows_dot(hid[col, :, lanes(p)], tok[col, :, cols(w)])
        for s in (1 - side, side):
            at = piece(k, s)
            mine = part[pl.ds(pl.multiple_of(s * sub, sub), sub), :]

            @pl.when(has_outer)
            def _():
                rs_copy(k, s, rs_r).wait_recv()
                out[at] = (mine + inc[(0, *at)].astype(F32)).astype(BF16)

            @pl.when(jnp.logical_not(has_outer))
            def _():
                out[at] = mine.astype(BF16)

            if s is side:
                @pl.when(jnp.logical_not(middle))
                def _():
                    rs_copy(k, s, rs_r).start()
            else:
                rs_start(k, s)

    def relayed(k, c):
        every = jnp.where(c == 0, RELAY[0], RELAY[1])
        return k % every == every // 2

    def spread(k, s):
        @pl.when(has_outer)
        def _():
            final(k, s, fo_s, outer).start()

    def spread_y(k, s):
        spread(k, s)

        @pl.when(jnp.logical_not(relayed(k, col)))
        def _():
            final_y(k, s).start()

    def cross(k):
        @pl.when(middle)
        def _():
            at = piece(k, side)
            rs_copy(k, side, fz_r).wait_recv()
            res[(col, *at)] = (out[at].astype(F32) + inc[(1, *at)].astype(F32)).astype(BF16)
            final(k, side, fc_s, inner).start()
            spread(k, side)
            final_y(k, side).start()

    def forward(k):
        final(k, 1 - side, fc_s, inner).wait_recv()
        spread_y(k, 1 - side)

    def forward_near(k):
        @pl.when(jnp.logical_not(middle))
        def _():
            final(k, side, fc_s, inner).wait_recv()
            spread_y(k, side)

    def relay(k, s, sem, dev):
        return moved(res, (1 - col, *piece(k, s)), sem, rz_r.at[k // min(RELAY), s], dev)

    def relay_out(k, s):
        @pl.when(has_outer)
        def _():
            relay(k, s, ro_s, outer).start()

    def relay_near(k):
        @pl.when(relayed(k, 1 - col))
        def _():
            @pl.when(middle)
            def _():
                moved(res, (1 - col, *piece(k, side)), fy_s, fy_r.at[k], other_y).wait_recv()
                relay(k, side, rc_s, inner).start()

            @pl.when(jnp.logical_not(middle))
            def _():
                relay(k, side, rc_s, inner).wait_recv()
            relay_out(k, side)

    def relay_far(k):
        @pl.when(relayed(k, 1 - col))
        def _():
            relay(k, 1 - side, rc_s, inner).wait_recv()
            relay_out(k, 1 - side)

    def take(k):
        p, w = where_is(k)
        at = (lanes(p), cols(w))

        @pl.when(jnp.logical_not(relayed(k, 1 - col)))
        def _():
            moved(res, (1 - col, *at), fy_s, fy_r.at[k], other_y).wait_recv()
        up_ref[cols(w), lanes(p)] = res[(0, *at)].T

    def grads_by(i):
        pace = jnp.where(has_outer, PACE, START)
        fast = 2 * START + jnp.where(i < 0, 0, PACE + pace * i)
        slow = 2 * START + 2 * PACE + i
        return jnp.minimum(panels, jnp.where(
            col == 1, jnp.minimum(fast, slow), START + 1 + i))

    def acts_by(i):
        return jnp.minimum(panels // 2, (grads_by(i + 1) + 2 - col) // 2)

    def when_in(i, end, body):
        @pl.when((i >= 0) & (i < end))
        def _():
            body(i)

    act(0)
    each(2, panels, own_square)
    load_rest.wait()

    @pl.when(col == 1)
    def _():
        each(0, START, pair)
        act(1)

    def ready(k):
        grad(k)

        @pl.when(col == 0)
        def _():
            pair(k)
    each(0, START, ready)

    @pl.when(col == 1)
    def _():
        y_move(1).start()

    def far_arrived(w):
        remote(tok.at[1 - col, own_t, cols(w)], tok.at[col, far_t, cols(w)], yt_s.at[w],
               yt_r.at[w], other_y).wait_recv()
        far_move(w).start()

    far_arrived(0)

    @pl.when(col == 0)
    def _():
        x_move.wait_recv()

    each(0, HOP, hop)
    far_move(0).wait_recv()

    each(2 - jnp.where(col == 0, 1, 0), acts_by(-1), act)
    each(START, grads_by(-1), grad)

    furthest = SPREAD + APART * (mid - 1)
    take_lag = furthest + max(TAKE, LATE + 2 * CROSS + 1 - SPREAD)

    def spreading(k):
        when_in(k - SPREAD - APART * depth, chunks, forward)
        when_in(k - CROSS - APART * depth, chunks, forward_near)
        when_in(k - CROSS, chunks, cross)
        when_in(k - LATE - APART * depth, chunks, relay_near)
        when_in(k - LATE - 2 * CROSS - APART * depth, chunks, relay_far)
        when_in(k - take_lag, chunks, take)

    def feed(i):
        @pl.when(col == 1)
        def _():
            when_in(i + HOP, panels, pair)
            when_in(i + HOP, panels, hop)
        each(acts_by(i - 1), acts_by(i), act)

        @pl.when(i == 0)
        def _():
            far_arrived(1)
        each(grads_by(i - 1), grads_by(i), grad)

        @pl.when(col == 0)
        def _():
            when_in(i + HOP, panels, pair)
            when_in(i + HOP, panels, hop)

    def main(i):
        @pl.when(has_outer)
        def _():
            feed(i)

        @pl.when(i == 1)
        def _():
            far_move(1).wait_recv()
        for n in range(2):
            @pl.when(i == 0)
            def _():
                arrive(n)
            if n == 0:
                @pl.when(i > 1)
                def _():
                    arrive(i)
            reduce(2 * i + n)
            spreading(2 * i + n)

            if n == 1:
                @pl.when(jnp.logical_not(has_outer))
                def _():
                    feed(i)

        @pl.when((col == 1) & (i >= panels // 2))
        def _():
            for n in range(2):
                gx_copy(2 * (i - panels // 2) + n).start()

    each(0, panels, main)
    load_wu.wait()
    strip = min(2 * LANES, width)

    def input_out(n):
        at = pl.ds(pl.multiple_of(n * strip, strip), strip)
        gi_out[:, at] = cols_dot(hid[0, own_ht, :], wu[at, :]).astype(BF16)
    def input_own(n):
        at = pl.ds(pl.multiple_of(n * strip, strip), strip)
        mine = cols_dot(hid[0, own_t, :], wu[at, :]).astype(BF16).astype(F32)
        gi_ref[:, at] = mine.astype(BF16)
    strips = width // strip
    gi_move = remote(gi_out, gi_in, gi_s, gi_r, other_tp)

    def finish(n):
        spreading(chunks + n)
        m = n - jnp.where(has_outer, SPREAD, 0)

        @pl.when((col == 1) & (m == 0))
        def _():
            moved(hid, (0, own_f), gx_s, gx_r, other_fs).wait_recv()

        for h in range(2):
            when_in(2 * m + h, strips, input_out)
        for h in range(2):
            when_in(2 * m + h - strips, strips, input_own)

        @pl.when(m == strips // 2 - 1)
        def _():
            gi_move.start()
    each(0, SPREAD + strips, finish)
    each(chunks + SPREAD + strips, chunks + take_lag, spreading)
    gi_move.wait_recv()
    gi_ref[...] = (gi_ref[...].astype(F32) + gi_in[...].astype(F32)).astype(BF16)

    for move in (y_move(0), y_move(1), cot_move, far_move(0), far_move(1), gi_move):
        move.wait_send()
    some = pl.ds(0, hidden // 2)
    remote(pa_out, pa_in, pa_s, pa_r.at[0], other_fs).wait_send()
    moved(hid, (1 - col, own_f), ya_s, ya_r.at[0], other_y).wait_send()
    moved(hid, (col, own_f), ox_s, act_r.at[0], other_fs).wait_send()
    moved(hid, (col, far_f), fx_s, act_r.at[0], other_fs).wait_send()
    @pl.when(col == 0)
    def _():
        x_move.wait_send()

    @pl.when(col == 1)
    def _():
        moved(hid, (0, own_f), gx_s, gx_r, other_fs).wait_send()

    @pl.when(middle)
    def _():
        remote(out.at[some], inc.at[1, some], rs_s, rs_r.at[0, 0], inner).wait_send()
        moved(res, (col, some), fc_s, fz_r.at[0, 0], inner).wait_send()

    @pl.when(jnp.logical_not(middle))
    def _():
        remote(out, inc.at[0], rs_s, rs_r.at[0, 0], inner).wait_send()

    @pl.when(has_outer)
    def _():
        moved(res, (col,), fo_s, fz_r.at[0, 0], outer).wait_send()

    def relay_sent(c):
        passed = [len(range(n // 2, chunks, n)) * sub // 2 for n in RELAY]

        @pl.when(middle)
        def _():
            kept = pl.ds(0, hidden - passed[c])
            moved(res, (c, kept), fy_s, fy_r.at[0], other_y).wait_send()
            some = pl.ds(0, passed[1 - c])
            moved(res, (1 - c, some), rc_s, rz_r.at[0, 0], inner).wait_send()

        @pl.when(jnp.logical_not(middle))
        def _():
            kept = pl.ds(0, hidden - 2 * passed[c])
            moved(res, (c, kept), fy_s, fy_r.at[0], other_y).wait_send()

        @pl.when(has_outer)
        def _():
            some = pl.ds(0, 2 * passed[1 - c])
            moved(res, (1 - c, some), ro_s, rz_r.at[0, 0], outer).wait_send()

    for c in range(2):
        @pl.when(col == c)
        def _():
            relay_sent(c)


def scale_kernel(factor, pieces, gi, up, res, gi_out, up_out, down_out, up_wide, down_wide,
                 sems, gi_sem):
    copies = [pltpu.make_async_copy(gi, gi_out, gi_sem)]
    copies[0].start()
    for i in range(pieces):
        for n, (src, wide, dst) in enumerate(
                ((up, up_wide, up_out), (res.at[1], down_wide, down_out))):
            rows = pl.ds(i * (src.shape[0] // pieces), src.shape[0] // pieces)
            wide[rows, :] = src[rows, :].astype(F32) * factor
            copy = pltpu.make_async_copy(wide.at[rows, :], dst.at[rows, :], sems.at[n, i])
            copy.start()
            copies.append(copy)
    for copy in copies:
        copy.wait()


def per_device(n_rep, inputs, pre_act, cotangent, up_weight, down_weight):
    half, width = inputs.shape
    hidden = pre_act.shape[1]
    panels = hidden // LANES
    dma = pltpu.SemaphoreType.DMA
    vmem = pl.BlockSpec(memory_space=pltpu.VMEM)
    anywhere = pl.BlockSpec(memory_space=pl.ANY)
    chunks = 2 * panels
    turn = turn_of(n_rep, chunks)
    one = dma((panels,))
    grad_inputs, grad_up, result = pl.pallas_call(
        functools.partial(kernel, n_rep),
        name="ffn_backward",
        out_shape=(
            pltpu.VMEM((half, width), BF16),
            pltpu.VMEM((width, hidden), BF16),
            pltpu.VMEM((2, hidden, width), BF16),
        ),
        in_specs=[anywhere] * 5,
        out_specs=(vmem, vmem, vmem),
        scratch_shapes=[
            pltpu.VMEM((half, hidden), BF16),
            pltpu.VMEM((width, hidden), BF16),
            pltpu.VMEM((hidden, width), BF16),
            pltpu.VMEM((2, 4 * half, width), BF16),
            pltpu.VMEM((2, 4 * half, hidden), BF16),
            pltpu.VMEM((half, hidden), F32),
            pltpu.VMEM((half, hidden), BF16),
            pltpu.VMEM((half, hidden), BF16),
            pltpu.VMEM((half, width), BF16),
            pltpu.VMEM((half, width), BF16),
            pltpu.VMEM((LANES, width // 2), F32),
            pltpu.VMEM((hidden, width), BF16),
            pltpu.VMEM((2, hidden, width), BF16),
            dma((6,)), dma((4,)), dma((4,)), dma((2,)), dma((2,)),
            dma, one, dma, dma, one, dma, dma,
            dma, one, dma, dma,
            dma, dma((turn, 2)), dma, dma, dma((turn, 2)), dma, dma((chunks,)),
            dma, dma, dma((-(-chunks // min(RELAY)), 2)),
        ],
        compiler_params=pltpu.CompilerParams(
            collective_id=0, has_side_effects=True, vmem_limit_bytes=48 * 2**20
        ),
    )(inputs, pre_act, cotangent, up_weight, down_weight)
    factor = (half * n_rep * lax.axis_size("tp")) ** (-0.5)
    pieces = 8
    return pl.pallas_call(
        functools.partial(scale_kernel, factor, pieces),
        name="scale_outputs",
        out_shape=(
            jax.ShapeDtypeStruct((half, width), BF16),
            jax.ShapeDtypeStruct((width, hidden), F32),
            jax.ShapeDtypeStruct((hidden, width), F32),
        ),
        in_specs=[vmem] * 3,
        out_specs=[anywhere] * 3,
        scratch_shapes=[
            pltpu.VMEM((width, hidden), F32),
            pltpu.VMEM((hidden, width), F32),
            dma((2, pieces)),
            dma,
        ],
        compiler_params=pltpu.CompilerParams(vmem_limit_bytes=40 * 2**20),
    )(*[pltpu.with_memory_space_constraint(g, pltpu.VMEM)
        for g in (grad_inputs, grad_up, result)])


def solution(mesh):
    assert mesh.shape["fs"] == 2 and mesh.shape["tp"] == 2 and mesh.shape["rep"] % 4 == 0
    placed = (
        P(("rep", "tp"), "fs"),
        P(("rep", "fs"), "tp"),
        P(("rep", "tp"), "fs"),
        P("fs", "tp"),
        P("tp", "fs"),
    )
    return jax.shard_map(
        functools.partial(per_device, mesh.shape["rep"]),
        mesh=mesh,
        in_specs=placed,
        out_specs=(P(("rep", "tp"), "fs"), P("fs", "tp"), P("tp", "fs")),
        check_vma=False,
    )
```

```python
import functools

import jax
import jax.numpy as jnp
from jax import lax
from jax.experimental import pallas as pl
from jax.experimental.pallas import tpu as pltpu
from jax.sharding import PartitionSpec as P

MESH = pl.DeviceIdType.MESH
LANES = 128
F32, BF16 = jnp.float32, jnp.bfloat16

START, HOP, PACE = 2, 2, 3
CROSS, SPREAD, APART, TAKE = 1, 3, 4, 6
RELAY, LATE = (32, 16), 11


def rows_dot(left, right):
    return lax.dot_general(left, right, (((0,), (0,)), ((), ())), preferred_element_type=F32)


def cols_dot(left, right):
    return lax.dot_general(left, right, (((1,), (1,)), ((), ())), preferred_element_type=F32)


def turn_of(n_rep, chunks):
    furthest = SPREAD + APART * (n_rep // 4 - 1)
    return min(chunks, 1 << (furthest + TAKE).bit_length())


def kernel(
    n_rep, x_hbm, pre_hbm, cot_hbm, wu_hbm, wd_hbm,
    gi_ref, up_ref, res,
    pre_ref, wu, wd, tok, hid, pa_own, pa_out, pa_in, gi_out, gi_in, part, out, inc,
    w_sem, tp_s, tp_r, yt_s, yt_r, ya_s, ya_r, ox_s, fx_s, act_r, gx_s, gx_r,
    pa_s, pa_r, gi_s, gi_r, rs_s, rs_r, fc_s, fo_s, fz_r, fy_s, fy_r, rc_s, ro_s, rz_r,
):
    half, hidden = pre_ref.shape
    width = wd.shape[1]
    panels = hidden // LANES
    sub, wide = LANES // 2, width // 2
    chunks = 2 * panels
    rep, fs, tp = lax.axis_index("rep"), lax.axis_index("fs"), lax.axis_index("tp")
    rows_n = n_rep // 2
    mid = rows_n // 2
    row, col = rep // 2, rep % 2
    side = jnp.where(row >= mid, 1, 0)
    depth = jnp.where(row >= mid, row - mid, mid - 1 - row)
    has_outer = depth < mid - 1
    middle = depth == 0
    step = 2 * side - 1

    def rep_at(r):
        return 2 * lax.rem(r + rows_n, rows_n) + col

    outer, inner = {"rep": rep_at(row + step)}, {"rep": rep_at(row - step)}
    other_y = {"rep": 2 * row + 1 - col}
    other_fs, other_tp = {"fs": 1 - fs}, {"tp": 1 - tp}

    def block(c, b):
        return pl.ds(pl.multiple_of((2 * c + b) * half, half), half)

    own_f, own_hf = block(col, fs), block(col, 1 - fs)
    far_f, far_hf = block(1 - col, fs), block(1 - col, 1 - fs)
    own_t, own_ht = block(col, tp), block(col, 1 - tp)
    far_t, far_ht = block(1 - col, tp), block(1 - col, 1 - tp)

    def remote(src, dst, s, r, dev):
        return pltpu.make_async_remote_copy(
            src_ref=src, dst_ref=dst, send_sem=s, recv_sem=r, device_id=dev,
            device_id_type=MESH)

    barrier = pltpu.get_barrier_semaphore()
    for dev in (outer, inner, other_y, other_fs, other_tp):
        pl.semaphore_signal(barrier, inc=1, device_id=dev, device_id_type=MESH)
    first = pl.ds(0, 2 * LANES)
    rest = pl.ds(2 * LANES, hidden - 2 * LANES)
    held = ((cot_hbm, tok.at[1, own_t]), (x_hbm, tok.at[0, own_t]), (pre_hbm, pre_ref),
            (wd_hbm.at[first], wd.at[first]), (wd_hbm.at[rest], wd.at[rest]), (wu_hbm, wu))
    loads = [pltpu.make_async_copy(src, dst, w_sem.at[i]) for i, (src, dst) in enumerate(held)]
    load_cot, load_x, load_pre, load_first, load_rest, load_wu = loads
    for load in loads[:4]:
        load.start()
    load_cot.wait()
    load_x.wait()
    pl.semaphore_wait(barrier, 5)

    def lanes(k):
        return pl.ds(pl.multiple_of(k * LANES, LANES), LANES)

    def where_is(k):
        early = k < 4
        return jnp.where(early, k % 2, k // 2), jnp.where(early, k // 2, k % 2)

    def cols(w):
        return pl.ds(pl.multiple_of(w * wide, wide), wide)

    def piece(k, s):
        p, w = where_is(k)
        return pl.ds(pl.multiple_of(p * LANES + s * sub, sub), sub), cols(w)

    turn = turn_of(n_rep, chunks)

    def moved(ref, at, s, r, dev):
        return remote(ref.at[at], ref.at[at], s, r, dev)

    def y_move(w):
        return moved(tok, (1 - col, own_t, cols(w)), yt_s.at[w], yt_r.at[w], other_y)

    def far_move(w):
        return moved(tok, (col, far_t, cols(w)), tp_s.at[2 + w], tp_r.at[2 + w], other_tp)

    y_move(0).start()
    cot_move = moved(tok, (1, own_t), tp_s.at[0], tp_r.at[0], other_tp)
    cot_move.start()
    x_move = moved(tok, (0, own_t), tp_s.at[1], tp_r.at[1], other_tp)

    @pl.when(col == 0)
    def _():
        x_move.start()

    def ya_copy(k):
        return moved(hid, (1 - col, own_f, lanes(k)), ya_s, ya_r.at[k], other_y)

    def ox_copy(k):
        return moved(hid, (col, own_f, lanes(k)), ox_s, act_r.at[k], other_fs)

    def fx_copy(k):
        return moved(hid, (col, far_f, lanes(k)), fx_s, act_r.at[k], other_fs)

    def gx_copy(k):
        return moved(hid, (0, own_f, lanes(k)), gx_s, gx_r, other_fs)

    def pa_copy(k):
        return remote(pa_out.at[:, lanes(k)], pa_in.at[:, lanes(k)], pa_s, pa_r.at[k],
                      other_fs)

    load_pre.wait()

    def each(lo, hi, body):
        def once(k, _):
            body(k)
            return 0
        lax.fori_loop(lo, hi, once, 0)

    def own_square(k):
        positive = jnp.maximum(pre_ref[:, lanes(k)].astype(F32), 0.0)
        hid[1, own_f, lanes(k)] = (positive * positive).astype(BF16)

        @pl.when(col == 0)
        def _():
            ya_copy(k).start()

    each(0, 2, own_square)

    @pl.when(col == 0)
    def _():
        y_move(1).start()
    load_rest.start()
    load_wu.start()
    load_first.wait()
    cot_move.wait_recv()

    def act(j):
        at = pl.ds(pl.multiple_of(j * 2 * LANES, 2 * LANES), 2 * LANES)
        for n in range(2):
            pa_out[:, lanes(2 * j + n)] = cols_dot(
                tok[1, own_hf, :], wd[lanes(2 * j + n), :]).astype(BF16)
            pa_copy(2 * j + n).start()
        pa_own[:, at] = cols_dot(tok[1, own_f, :], wd[at, :])

    def pair(k):
        ox_copy(k).start()

    def grad(k):
        pa_copy(k).wait_recv()
        positive = jnp.maximum(pre_ref[:, lanes(k)].astype(F32), 0.0)
        total = pa_own[:, lanes(k)] + pa_in[:, lanes(k)].astype(F32)
        hid[0, own_f, lanes(k)] = (2.0 * positive * total).astype(BF16)

        @pl.when(col == 1)
        def _():
            ya_copy(k).start()

    def hop(k):
        remote(hid.at[1 - col, own_f, lanes(k)], hid.at[col, far_f, lanes(k)], ya_s,
               ya_r.at[k], other_y).wait_recv()
        fx_copy(k).start()

    def rs_copy(k, s, recv):
        slot = jnp.where(middle, 1, 0)
        return remote(out.at[piece(k, s)], inc.at[(slot, *piece(k, s))], rs_s,
                      recv.at[k % turn, s], inner)

    def rs_start(k, s):
        @pl.when(middle)
        def _():
            rs_copy(k, s, fz_r).start()

        @pl.when(jnp.logical_not(middle))
        def _():
            rs_copy(k, s, rs_r).start()

    def final(k, s, sem, dev):
        return moved(res, (col, *piece(k, s)), sem, fz_r.at[k % turn, s], dev)

    def final_y(k, s):
        return moved(res, (col, *piece(k, s)), fy_s, fy_r.at[k], other_y)

    def arrive(k):
        moved(hid, (col, pl.ds(0, 2 * half), lanes(k)), ox_s, act_r.at[k], other_fs).wait_recv()

    def reduce(k):
        p, w = where_is(k)
        part[...] = rows_dot(hid[col, :, lanes(p)], tok[col, :, cols(w)])
        for s in (1 - side, side):
            at = piece(k, s)
            mine = part[pl.ds(pl.multiple_of(s * sub, sub), sub), :]

            @pl.when(has_outer)
            def _():
                rs_copy(k, s, rs_r).wait_recv()
                out[at] = (mine + inc[(0, *at)].astype(F32)).astype(BF16)

            @pl.when(jnp.logical_not(has_outer))
            def _():
                out[at] = mine.astype(BF16)

            if s is side:
                @pl.when(jnp.logical_not(middle))
                def _():
                    rs_copy(k, s, rs_r).start()
            else:
                rs_start(k, s)

    def relayed(k, c):
        every = jnp.where(c == 0, RELAY[0], RELAY[1])
        return k % every == every // 2

    def spread(k, s):
        @pl.when(has_outer)
        def _():
            final(k, s, fo_s, outer).start()

    def spread_y(k, s):
        spread(k, s)

        @pl.when(jnp.logical_not(relayed(k, col)))
        def _():
            final_y(k, s).start()

    def cross(k):
        @pl.when(middle)
        def _():
            at = piece(k, side)
            rs_copy(k, side, fz_r).wait_recv()
            res[(col, *at)] = (out[at].astype(F32) + inc[(1, *at)].astype(F32)).astype(BF16)
            final(k, side, fc_s, inner).start()
            spread(k, side)
            final_y(k, side).start()

    def forward(k):
        final(k, 1 - side, fc_s, inner).wait_recv()
        spread_y(k, 1 - side)

    def forward_near(k):
        @pl.when(jnp.logical_not(middle))
        def _():
            final(k, side, fc_s, inner).wait_recv()
            spread_y(k, side)

    def relay(k, s, sem, dev):
        return moved(res, (1 - col, *piece(k, s)), sem, rz_r.at[k // min(RELAY), s], dev)

    def relay_out(k, s):
        @pl.when(has_outer)
        def _():
            relay(k, s, ro_s, outer).start()

    def relay_near(k):
        @pl.when(relayed(k, 1 - col))
        def _():
            @pl.when(middle)
            def _():
                moved(res, (1 - col, *piece(k, side)), fy_s, fy_r.at[k], other_y).wait_recv()
                relay(k, side, rc_s, inner).start()

            @pl.when(jnp.logical_not(middle))
            def _():
                relay(k, side, rc_s, inner).wait_recv()
            relay_out(k, side)

    def relay_far(k):
        @pl.when(relayed(k, 1 - col))
        def _():
            relay(k, 1 - side, rc_s, inner).wait_recv()
            relay_out(k, 1 - side)

    def take(k):
        p, w = where_is(k)
        at = (lanes(p), cols(w))

        @pl.when(jnp.logical_not(relayed(k, 1 - col)))
        def _():
            moved(res, (1 - col, *at), fy_s, fy_r.at[k], other_y).wait_recv()
        up_ref[cols(w), lanes(p)] = res[(0, *at)].T

    def grads_by(i):
        pace = jnp.where(has_outer, PACE, START)
        fast = 2 * START + jnp.where(i < 0, 0, START + pace * i)
        slow = 2 * START + 2 * PACE + i
        return jnp.minimum(panels, jnp.where(
            col == 1, jnp.minimum(fast, slow), START + 1 + i))

    def acts_by(i):
        return jnp.minimum(panels // 2, (grads_by(i + 1) + 2 - col) // 2)

    def when_in(i, end, body):
        @pl.when((i >= 0) & (i < end))
        def _():
            body(i)

    act(0)
    each(2, panels, own_square)
    load_rest.wait()

    @pl.when(col == 1)
    def _():
        each(0, START, pair)
        act(1)

    def ready(k):
        grad(k)

        @pl.when(col == 0)
        def _():
            pair(k)
    each(0, START, ready)

    @pl.when(col == 1)
    def _():
        y_move(1).start()

    def far_arrived(w):
        remote(tok.at[1 - col, own_t, cols(w)], tok.at[col, far_t, cols(w)], yt_s.at[w],
               yt_r.at[w], other_y).wait_recv()
        far_move(w).start()

    far_arrived(0)

    @pl.when(col == 0)
    def _():
        x_move.wait_recv()

    each(0, HOP, hop)
    far_move(0).wait_recv()

    each(2 - jnp.where(col == 0, 1, 0), acts_by(-1), act)
    each(START, grads_by(-1), grad)

    furthest = SPREAD + APART * (mid - 1)
    take_lag = furthest + max(TAKE, LATE + 2 * CROSS + 1 - SPREAD)

    def spreading(k):
        when_in(k - SPREAD - APART * depth, chunks, forward)
        when_in(k - CROSS - APART * depth, chunks, forward_near)
        when_in(k - CROSS, chunks, cross)
        when_in(k - LATE - APART * depth, chunks, relay_near)
        when_in(k - LATE - 2 * CROSS - APART * depth, chunks, relay_far)
        when_in(k - take_lag, chunks, take)

    def feed(i):
        @pl.when(col == 1)
        def _():
            when_in(i + HOP, panels, pair)
            when_in(i + HOP, panels, hop)
        each(acts_by(i - 1), acts_by(i), act)

        @pl.when(i == 0)
        def _():
            far_arrived(1)
        each(grads_by(i - 1), grads_by(i), grad)

        @pl.when(col == 0)
        def _():
            when_in(i + HOP, panels, pair)
            when_in(i + HOP, panels, hop)

    def main(i):
        @pl.when(has_outer)
        def _():
            feed(i)

        @pl.when(i == 1)
        def _():
            far_move(1).wait_recv()
        for n in range(2):
            @pl.when(i == 0)
            def _():
                arrive(n)
            if n == 0:
                @pl.when(i > 1)
                def _():
                    arrive(i)
            reduce(2 * i + n)
            spreading(2 * i + n)

            if n == 1:
                @pl.when(jnp.logical_not(has_outer))
                def _():
                    feed(i)

        @pl.when((col == 1) & (i >= panels // 2))
        def _():
            for n in range(2):
                gx_copy(2 * (i - panels // 2) + n).start()

    each(0, panels, main)
    load_wu.wait()
    strip = min(2 * LANES, width)

    def input_out(n):
        at = pl.ds(pl.multiple_of(n * strip, strip), strip)
        gi_out[:, at] = cols_dot(hid[0, own_ht, :], wu[at, :]).astype(BF16)
    def input_own(n):
        at = pl.ds(pl.multiple_of(n * strip, strip), strip)
        mine = cols_dot(hid[0, own_t, :], wu[at, :]).astype(BF16).astype(F32)
        gi_ref[:, at] = mine.astype(BF16)
    strips = width // strip
    gi_move = remote(gi_out, gi_in, gi_s, gi_r, other_tp)

    def finish(n):
        spreading(chunks + n)
        m = n - jnp.where(has_outer, SPREAD, 0)

        @pl.when((col == 1) & (m == 0))
        def _():
            moved(hid, (0, own_f), gx_s, gx_r, other_fs).wait_recv()

        for h in range(2):
            when_in(2 * m + h, strips, input_out)
        for h in range(2):
            when_in(2 * m + h - strips, strips, input_own)

        @pl.when(m == strips // 2 - 1)
        def _():
            gi_move.start()
    each(0, SPREAD + strips, finish)
    each(chunks + SPREAD + strips, chunks + take_lag, spreading)
    gi_move.wait_recv()
    gi_ref[...] = (gi_ref[...].astype(F32) + gi_in[...].astype(F32)).astype(BF16)

    for move in (y_move(0), y_move(1), cot_move, far_move(0), far_move(1), gi_move):
        move.wait_send()
    some = pl.ds(0, hidden // 2)
    remote(pa_out, pa_in, pa_s, pa_r.at[0], other_fs).wait_send()
    moved(hid, (1 - col, own_f), ya_s, ya_r.at[0], other_y).wait_send()
    moved(hid, (col, own_f), ox_s, act_r.at[0], other_fs).wait_send()
    moved(hid, (col, far_f), fx_s, act_r.at[0], other_fs).wait_send()
    @pl.when(col == 0)
    def _():
        x_move.wait_send()

    @pl.when(col == 1)
    def _():
        moved(hid, (0, own_f), gx_s, gx_r, other_fs).wait_send()

    @pl.when(middle)
    def _():
        remote(out.at[some], inc.at[1, some], rs_s, rs_r.at[0, 0], inner).wait_send()
        moved(res, (col, some), fc_s, fz_r.at[0, 0], inner).wait_send()

    @pl.when(jnp.logical_not(middle))
    def _():
        remote(out, inc.at[0], rs_s, rs_r.at[0, 0], inner).wait_send()

    @pl.when(has_outer)
    def _():
        moved(res, (col,), fo_s, fz_r.at[0, 0], outer).wait_send()

    def relay_sent(c):
        passed = [len(range(n // 2, chunks, n)) * sub // 2 for n in RELAY]

        @pl.when(middle)
        def _():
            kept = pl.ds(0, hidden - passed[c])
            moved(res, (c, kept), fy_s, fy_r.at[0], other_y).wait_send()
            some = pl.ds(0, passed[1 - c])
            moved(res, (1 - c, some), rc_s, rz_r.at[0, 0], inner).wait_send()

        @pl.when(jnp.logical_not(middle))
        def _():
            kept = pl.ds(0, hidden - 2 * passed[c])
            moved(res, (c, kept), fy_s, fy_r.at[0], other_y).wait_send()

        @pl.when(has_outer)
        def _():
            some = pl.ds(0, 2 * passed[1 - c])
            moved(res, (1 - c, some), ro_s, rz_r.at[0, 0], outer).wait_send()

    for c in range(2):
        @pl.when(col == c)
        def _():
            relay_sent(c)


def scale_kernel(factor, pieces, gi, up, res, gi_out, up_out, down_out, up_wide, down_wide,
                 sems, gi_sem):
    copies = [pltpu.make_async_copy(gi, gi_out, gi_sem)]
    copies[0].start()
    for i in range(pieces):
        for n, (src, wide, dst) in enumerate(
                ((up, up_wide, up_out), (res.at[1], down_wide, down_out))):
            rows = pl.ds(i * (src.shape[0] // pieces), src.shape[0] // pieces)
            wide[rows, :] = src[rows, :].astype(F32) * factor
            copy = pltpu.make_async_copy(wide.at[rows, :], dst.at[rows, :], sems.at[n, i])
            copy.start()
            copies.append(copy)
    for copy in copies:
        copy.wait()


def per_device(n_rep, inputs, pre_act, cotangent, up_weight, down_weight):
    half, width = inputs.shape
    hidden = pre_act.shape[1]
    panels = hidden // LANES
    dma = pltpu.SemaphoreType.DMA
    vmem = pl.BlockSpec(memory_space=pltpu.VMEM)
    anywhere = pl.BlockSpec(memory_space=pl.ANY)
    chunks = 2 * panels
    turn = turn_of(n_rep, chunks)
    one = dma((panels,))
    grad_inputs, grad_up, result = pl.pallas_call(
        functools.partial(kernel, n_rep),
        name="ffn_backward",
        out_shape=(
            pltpu.VMEM((half, width), BF16),
            pltpu.VMEM((width, hidden), BF16),
            pltpu.VMEM((2, hidden, width), BF16),
        ),
        in_specs=[anywhere] * 5,
        out_specs=(vmem, vmem, vmem),
        scratch_shapes=[
            pltpu.VMEM((half, hidden), BF16),
            pltpu.VMEM((width, hidden), BF16),
            pltpu.VMEM((hidden, width), BF16),
            pltpu.VMEM((2, 4 * half, width), BF16),
            pltpu.VMEM((2, 4 * half, hidden), BF16),
            pltpu.VMEM((half, hidden), F32),
            pltpu.VMEM((half, hidden), BF16),
            pltpu.VMEM((half, hidden), BF16),
            pltpu.VMEM((half, width), BF16),
            pltpu.VMEM((half, width), BF16),
            pltpu.VMEM((LANES, width // 2), F32),
            pltpu.VMEM((hidden, width), BF16),
            pltpu.VMEM((2, hidden, width), BF16),
            dma((6,)), dma((4,)), dma((4,)), dma((2,)), dma((2,)),
            dma, one, dma, dma, one, dma, dma,
            dma, one, dma, dma,
            dma, dma((turn, 2)), dma, dma, dma((turn, 2)), dma, dma((chunks,)),
            dma, dma, dma((-(-chunks // min(RELAY)), 2)),
        ],
        compiler_params=pltpu.CompilerParams(
            collective_id=0, has_side_effects=True, vmem_limit_bytes=48 * 2**20
        ),
    )(inputs, pre_act, cotangent, up_weight, down_weight)
    factor = (half * n_rep * lax.axis_size("tp")) ** (-0.5)
    pieces = 8
    return pl.pallas_call(
        functools.partial(scale_kernel, factor, pieces),
        name="scale_outputs",
        out_shape=(
            jax.ShapeDtypeStruct((half, width), BF16),
            jax.ShapeDtypeStruct((width, hidden), F32),
            jax.ShapeDtypeStruct((hidden, width), F32),
        ),
        in_specs=[vmem] * 3,
        out_specs=[anywhere] * 3,
        scratch_shapes=[
            pltpu.VMEM((width, hidden), F32),
            pltpu.VMEM((hidden, width), F32),
            dma((2, pieces)),
            dma,
        ],
        compiler_params=pltpu.CompilerParams(vmem_limit_bytes=40 * 2**20),
    )(*[pltpu.with_memory_space_constraint(g, pltpu.VMEM)
        for g in (grad_inputs, grad_up, result)])


def solution(mesh):
    assert mesh.shape["fs"] == 2 and mesh.shape["tp"] == 2 and mesh.shape["rep"] % 4 == 0
    placed = (
        P(("rep", "tp"), "fs"),
        P(("rep", "fs"), "tp"),
        P(("rep", "tp"), "fs"),
        P("fs", "tp"),
        P("tp", "fs"),
    )
    return jax.shard_map(
        functools.partial(per_device, mesh.shape["rep"]),
        mesh=mesh,
        in_specs=placed,
        out_specs=(P(("rep", "tp"), "fs"), P("fs", "tp"), P("tp", "fs")),
        check_vma=False,
    )
```
